256 devices in a mesh: sp: 64 (over z, x, core), tp: 4 (over y).
Axes of the slice: x: 4, y: 4, z: 8, core: 2. Of those that a mesh axis runs over, the one named last changes fastest.
Arguments:
- incoming_residual_stream: bfloat16 [32768, 2048], P(('sp', 'tp')), may hold values from -6 to 6
- result_valve: bfloat16 [32768, 2048], P('sp', 'tp'), may hold values from -6 to 6
- channel_feed_matrix: bfloat16 [32768, 2048], P('sp', 'tp'), may hold values from -6 to 6
- memory_feed_matrix: bfloat16 [32768, 512], P('sp', 'tp'), may hold values from -6 to 6
- memory_query_matrix: bfloat16 [32768, 512], P('sp', 'tp'), may hold values from -6 to 6
- unsoftened_deltas: float32 [32768, 32], P('sp', 'tp'), may hold values from -2.7 to 2.7
- delta_offset: float32 [32], P('tp'), may hold values from -4.5 to -3.5
- channel_fading_speed: float32 [32], P('tp'), as said below
- extra_log_fading: float32 [32768, 32], P('sp', 'tp'), may hold values from -0.7 to 0
- bypass_factor: float32 [32], P('tp'), may hold values from 0.1 to 1.9
- channel_feed_kernel: bfloat16 [4, 2048], P(None, 'tp'), may hold values from -3 to 3
- memory_feed_kernel: bfloat16 [4, 512], P(None, 'tp'), may hold values from -3 to 3
- memory_query_kernel: bfloat16 [4, 512], P(None, 'tp'), may hold values from -3 to 3
- cluster_scaling_vector: float32 [2048], P('tp'), may hold values from 0.1 to 1.9
- mixer_result_matrix: bfloat16 [2048, 2048], P('tp'), may hold values from -0.125 to 0.125
- initial_scaling_vector: float32 [2048], replicated, may hold values from 0.1 to 1.9
- valve_matrix: bfloat16 [2048, 5632], P('sp', 'tp'), may hold values from -0.125 to 0.125
- widen_matrix: bfloat16 [2048, 5632], P('sp', 'tp'), may hold values from -0.125 to 0.125
- shrink_matrix: bfloat16 [5632, 2048], P('tp', 'sp'), may hold values from -0.078125 to 0.078125
- valve_filter_kernel: bfloat16 [3, 5632], P(None, 'tp'), may hold values from -3.5 to 3.5
- widen_filter_kernel: bfloat16 [3, 5632], P(None, 'tp'), may hold values from -3.5 to 3.5
- latter_scaling_vector: float32 [2048], replicated, may hold values from 0.1 to 1.9
Outputs:
- layer_out: bfloat16 [32768, 2048], P(('sp', 'tp'))
The draws below stay inside these ranges and needn't reach their ends.
Inputs may be any that keep to these rules, and one draw needn't show every extreme that they name: `channel_fading_speed`: positive.
All inputs are finite; a program needn't handle non-finite values.
Results may differ from the reference program's by a relative error of at most 0.02.
Values may be sent and summed in bfloat16 or wider, within the bound.
A program may use at most 128 MiB of HBM per device.

```python
import math
import jax
import jax.numpy as jnp
from jax import lax

D = 2048
HEADS = 32
HEAD_DIM = 64
GROUPS = 4
STATE = 128
FF = 5632
CONV = 4
FCONV = 3
BLOCK = 128
TOK_DEV = 512
INNER = 2048
TOKENS = 32768
N_TP = 4


def draw_unsoftened_deltas(key, part):
    noise_key = jax.random.fold_in(key, 11)
    block_key = jax.random.fold_in(key, 12)
    centred_part = jnp.clip(0.5 * jax.random.normal(noise_key, (TOKENS, HEADS), jnp.float32), -2.0, 2.0)
    shifts = jax.random.uniform(block_key, (TOKENS // TOK_DEV, 1), jnp.float32, -0.7, 0.7)
    return centred_part + jnp.repeat(shifts, TOK_DEV, axis=0)


def draw_channel_fading_speed(key, part):
    slow_share = 0.5
    slow_mask = jax.random.uniform(jax.random.fold_in(key, 21), (HEADS,), jnp.float32) < slow_share
    fast_rate = jnp.exp(jax.random.uniform(jax.random.fold_in(key, 22), (HEADS,), jnp.float32, 0.0, math.log(4.0)))
    slow_rate = jax.random.uniform(jax.random.fold_in(key, 23), (HEADS,), jnp.float32, 10.0, 30.0) / TOKENS
    return jnp.where(slow_mask, slow_rate, fast_rate)


def draw_extra_log_fading(key, part):
    hits = jax.random.uniform(jax.random.fold_in(key, 31), (TOKENS, HEADS), jnp.float32) < 4.0 / TOKENS
    drops = jnp.log(jax.random.uniform(jax.random.fold_in(key, 32), (TOKENS, HEADS), jnp.float32, 0.5, 0.8))
    return jnp.where(hits, drops, 0.0)


def block_levels(key, dims, cuts, least, largest):
    level = 1.0
    for axis_at, shards_of in cuts:
        heights = jax.random.uniform(jax.random.fold_in(jax.random.fold_in(key, 6), axis_at), (shards_of,), jnp.float32, least / len(cuts), largest / len(cuts))
        level = level * jnp.repeat(jnp.exp(heights), dims[axis_at] // shards_of).reshape((-1,) + (1,) * (len(dims) - 1 - axis_at))
    return level


def noise(rng, dims, scale, limit, cuts=(), held_as=jnp.bfloat16):
    result = jax.random.normal(rng, dims, jnp.float32) * scale
    if len(cuts) > 0:
        result = block_levels(rng, dims, cuts, -0.22, 0.18) * result
    return jnp.clip(result, min=-limit, max=limit).astype(held_as)


def setup_inputs(seed: int = 0) -> dict:
    keys = jax.random.split(jax.random.key(seed), 23)
    incoming_residual_stream = noise(keys[0], (TOKENS, D), 1.0, 6.0, ((0, 256),))
    result_valve = noise(keys[1], (TOKENS, INNER), 1.0, 6.0, ((0, 64), (1, 4)))
    channel_feed_matrix = noise(keys[2], (TOKENS, INNER), 1.0, 6.0, ((0, 64), (1, 4)))
    memory_feed_matrix = noise(keys[3], (TOKENS, GROUPS * STATE), 1.0, 6.0, ((0, 64), (1, 4)))
    memory_query_matrix = noise(keys[4], (TOKENS, GROUPS * STATE), 1.0, 6.0, ((0, 64), (1, 4)))
    unsoftened_deltas = draw_unsoftened_deltas(jax.random.fold_in(keys[22], 71), 0)
    delta_offset = jnp.clip(-4.5 + 1.0 * jax.random.uniform(keys[6], (HEADS,), jnp.float32) ** block_levels(keys[6], (HEADS,), ((0, 4),), -0.2, 0.2), -4.5, -3.5)
    channel_fading_speed = draw_channel_fading_speed(jax.random.fold_in(keys[22], 71), 0)
    extra_log_fading = draw_extra_log_fading(jax.random.fold_in(keys[22], 71), 0)
    bypass_factor = jnp.clip(1.0 + 0.18 * jax.random.normal(keys[9], (HEADS,), jnp.float32), 0.1, 1.9)
    channel_feed_kernel = noise(keys[10], (CONV, INNER), CONV ** -0.5, 3.0, ((1, 4),))
    memory_feed_kernel = noise(keys[11], (CONV, GROUPS * STATE), CONV ** -0.5, 3.0, ((1, 4),))
    memory_query_kernel = noise(keys[12], (CONV, GROUPS * STATE), CONV ** -0.5, 3.0, ((1, 4),))
    cluster_scaling_vector = jnp.clip(1.0 + 0.18 * jax.random.normal(keys[13], (INNER,), jnp.float32), 0.1, 1.9)
    mixer_result_matrix = noise(keys[14], (INNER, D), INNER ** -0.5, 0.125, ((0, 4),))
    initial_scaling_vector = jnp.clip(1.0 + 0.18 * jax.random.normal(keys[15], (D,), jnp.float32), 0.1, 1.9)
    valve_matrix = noise(keys[16], (D, FF), D ** -0.5, 0.125, ((0, 64), (1, 4)))
    widen_matrix = noise(keys[17], (D, FF), D ** -0.5, 0.125, ((0, 64), (1, 4)))
    shrink_matrix = noise(keys[18], (FF, D), FF ** -0.5, 0.078125, ((0, 4), (1, 64)))
    valve_filter_kernel = noise(keys[19], (FCONV, FF), FCONV ** -0.5, 3.5, ((1, 4),))
    widen_filter_kernel = noise(keys[20], (FCONV, FF), FCONV ** -0.5, 3.5, ((1, 4),))
    latter_scaling_vector = jnp.clip(1.0 + 0.18 * jax.random.normal(keys[21], (D,), jnp.float32), 0.1, 1.9)
    return {"incoming_residual_stream": incoming_residual_stream, "result_valve": result_valve, "channel_feed_matrix": channel_feed_matrix, "memory_feed_matrix": memory_feed_matrix, "memory_query_matrix": memory_query_matrix, "unsoftened_deltas": unsoftened_deltas, "delta_offset": delta_offset, "channel_fading_speed": channel_fading_speed, "extra_log_fading": extra_log_fading, "bypass_factor": bypass_factor, "channel_feed_kernel": channel_feed_kernel, "memory_feed_kernel": memory_feed_kernel, "memory_query_kernel": memory_query_kernel, "cluster_scaling_vector": cluster_scaling_vector, "mixer_result_matrix": mixer_result_matrix, "initial_scaling_vector": initial_scaling_vector, "valve_matrix": valve_matrix, "widen_matrix": widen_matrix, "shrink_matrix": shrink_matrix, "valve_filter_kernel": valve_filter_kernel, "widen_filter_kernel": widen_filter_kernel, "latter_scaling_vector": latter_scaling_vector}


EPSILON = 1e-05
ALPHA = 2.0 ** 0.25
HIGHEST = lax.Precision.HIGHEST

def causal_conv(signal, before, tap_weights):
    tap_count = tap_weights.shape[0]
    row_count = signal.shape[0]
    padded = jnp.concatenate([before, signal], axis=0).astype(jnp.float32)
    running = jnp.zeros(signal.shape, jnp.float32)
    for tap_index in range(tap_count):
        running = running + tap_weights[tap_index].astype(jnp.float32) * padded[tap_index:tap_index + row_count]
    return running

def zero_rim(signal, tap_count):
    return jnp.zeros((tap_count - 1, signal.shape[1]), signal.dtype)

def layer_norm(values, scales):
    row_mean = lax.optimization_barrier(jnp.mean(values, axis=-1, keepdims=True))
    centred = values - row_mean
    spread = lax.optimization_barrier(jnp.mean(centred * centred, axis=-1, keepdims=True))
    return centred * lax.rsqrt(spread + EPSILON) * scales

def block_sum(activations, weights, pieces):
    slice_width = activations.shape[1] // pieces
    running = jnp.zeros((activations.shape[0], weights.shape[1]), jnp.float32)
    for piece_index in range(pieces):
        lower = piece_index * slice_width
        partial_value = jnp.dot(activations[:, lower:lower + slice_width], weights[lower:lower + slice_width], preferred_element_type=jnp.float32)
        rounded = lax.optimization_barrier(partial_value.astype(jnp.bfloat16))
        running = running + rounded.astype(jnp.float32)
    return running

def ssd_block(state_now, inputs):
    x_blk, b_blk, c_blk, decay_blk = inputs
    cum_decay = jnp.cumsum(decay_blk, axis=0)
    block_len = decay_blk.shape[0]
    causal = jnp.tril(jnp.ones((block_len, block_len), dtype=bool))
    between = cum_decay[:, None] - cum_decay[None, :]
    lag = jnp.exp(jnp.where(causal[:, :, None, None], between, -jnp.inf))
    affinity = jnp.einsum('lgn,sgn->lsg', c_blk, b_blk, precision=HIGHEST)
    mixing = affinity[..., None] * lag
    within = jnp.einsum('lsgh,sghp->lghp', mixing, x_blk, precision=HIGHEST)
    carried = jnp.einsum('lgn,ghpn->lghp', c_blk, state_now, precision=HIGHEST) * jnp.exp(cum_decay)[..., None]
    to_end = jnp.exp(cum_decay[-1] - cum_decay)
    fresh = jnp.einsum('lgn,lghp->ghpn', b_blk, x_blk * to_end[..., None], precision=HIGHEST)
    state_next = state_now * jnp.exp(cum_decay[-1])[..., None, None] + fresh
    return (state_next, within + carried)

def reference(incoming_residual_stream, result_valve, channel_feed_matrix, memory_feed_matrix, memory_query_matrix, unsoftened_deltas, delta_offset, channel_fading_speed, extra_log_fading, bypass_factor, channel_feed_kernel, memory_feed_kernel, memory_query_kernel, cluster_scaling_vector, mixer_result_matrix, initial_scaling_vector, valve_matrix, widen_matrix, shrink_matrix, valve_filter_kernel, widen_filter_kernel, latter_scaling_vector):
    group_heads = HEADS // GROUPS
    x_act = jax.nn.silu(causal_conv(channel_feed_matrix, zero_rim(channel_feed_matrix, CONV), channel_feed_kernel)).astype(jnp.bfloat16)
    b_act = jax.nn.silu(causal_conv(memory_feed_matrix, zero_rim(memory_feed_matrix, CONV), memory_feed_kernel)).astype(jnp.bfloat16)
    c_act = jax.nn.silu(causal_conv(memory_query_matrix, zero_rim(memory_query_matrix, CONV), memory_query_kernel)).astype(jnp.bfloat16)
    channel_delta_amount = jax.nn.softplus(unsoftened_deltas + delta_offset[None, :])
    log_fading_amount = extra_log_fading - channel_fading_speed[None, :] * channel_delta_amount
    block_count = TOKENS // BLOCK
    x_heads = x_act.astype(jnp.float32).reshape(TOKENS, GROUPS, group_heads, HEAD_DIM)
    x_scaled = x_heads * channel_delta_amount.reshape(TOKENS, GROUPS, group_heads)[..., None]
    x_blocks = x_scaled.reshape(block_count, BLOCK, GROUPS, group_heads, HEAD_DIM)
    b_blocks = b_act.astype(jnp.float32).reshape(block_count, BLOCK, GROUPS, STATE)
    c_blocks = c_act.astype(jnp.float32).reshape(block_count, BLOCK, GROUPS, STATE)
    decay_blocks = log_fading_amount.reshape(block_count, BLOCK, GROUPS, group_heads)
    initial = jnp.zeros((GROUPS, group_heads, HEAD_DIM, STATE), jnp.float32)
    _, mixed = lax.scan(ssd_block, initial, (x_blocks, b_blocks, c_blocks, decay_blocks))
    y_heads = mixed.reshape(TOKENS, GROUPS, group_heads, HEAD_DIM)
    y_heads = y_heads + bypass_factor.reshape(GROUPS, group_heads)[None, :, :, None] * x_heads
    gated = y_heads.reshape(TOKENS, GROUPS, INNER // GROUPS)
    gated = gated * jax.nn.silu(result_valve.astype(jnp.float32)).reshape(TOKENS, GROUPS, INNER // GROUPS)
    gated = gated * lax.rsqrt(lax.optimization_barrier(jnp.mean(gated * gated, axis=-1, keepdims=True)) + EPSILON)
    y_norm = (gated.reshape(TOKENS, INNER) * cluster_scaling_vector[None, :]).astype(jnp.bfloat16)
    mixer = block_sum(y_norm, mixer_result_matrix, N_TP)
    normed = layer_norm(ALPHA * incoming_residual_stream.astype(jnp.float32) + mixer, initial_scaling_vector).astype(jnp.bfloat16)
    gate_proj = jnp.dot(normed, valve_matrix, preferred_element_type=jnp.float32).astype(jnp.bfloat16)
    up_proj = jnp.dot(normed, widen_matrix, preferred_element_type=jnp.float32).astype(jnp.bfloat16)
    gate_conv = causal_conv(gate_proj, zero_rim(gate_proj, FCONV), valve_filter_kernel)
    up_conv = causal_conv(up_proj, zero_rim(up_proj, FCONV), widen_filter_kernel)
    hidden = (jax.nn.silu(gate_conv) * up_conv).astype(jnp.bfloat16)
    channel = block_sum(hidden, shrink_matrix, N_TP)
    return layer_norm(ALPHA * normed.astype(jnp.float32) + channel, latter_scaling_vector).astype(jnp.bfloat16)
```

```python
import jax
import jax.numpy as jnp
from jax import lax
from jax.experimental import pallas as pl
from jax.experimental.pallas import tpu as pltpu
from jax.sharding import Mesh
from jax.sharding import PartitionSpec as P

HEADS = 8
HEAD_DIM = 64
STATE = 128
BLOCK = 128
BLOCKS = 4
ROWS = BLOCK * BLOCKS
INNER = 512
D = 2048
FF = 1408
COLS = 3 * FF
NA = 1664
EPSILON = 1e-05
ALPHA = 2.0**0.25
SP = ("sp_0", "sp_1", "sp_2")
SP_TP = ("sp_0", "sp_1", "sp_2", "tp")
MESH = pl.DeviceIdType.MESH
F32 = jnp.float32
BF16 = jnp.bfloat16
NT = (((1,), (1,)), ((), ()))


def wrap(value, count):
    return lax.rem(value + 2 * count, count)


class Wire:
    def __init__(self, send_sem):
        self.send_sem = send_sem
        self.count = 0
        self.waits = []

    def send(self, src, dst, dev, recv_sem, when=None):
        copy = pltpu.make_async_remote_copy(
            src_ref=src,
            dst_ref=dst,
            send_sem=self.send_sem.at[self.count],
            recv_sem=recv_sem,
            device_id=dev,
            device_id_type=MESH,
        )
        self.count += 1
        if when is None:
            copy.start()
        else:
            pl.when(when)(copy.start)
        self.waits.append((copy, when))

    def arrive(self, dst, recv_sem, dev):
        pltpu.make_async_remote_copy(
            src_ref=dst,
            dst_ref=dst,
            send_sem=self.send_sem.at[0],
            recv_sem=recv_sem,
            device_id=dev,
            device_id_type=MESH,
        ).wait_recv()

    def finish(self):
        for copy, when in self.waits:
            if when is None:
                copy.wait_send()
            else:
                pl.when(when)(copy.wait_send)


def weight_gather(wire, wv, rsem, psem, ids):
    z, x, c, _ = ids
    cols_a, cols_b = pl.ds(0, NA), pl.ds(NA, COLS - NA)
    half, whole = (pl.ds(0, 16), pl.ds(16, 16)), pl.ds(0, 32)
    zp, zm = {"sp_0": wrap(z + 1, 8)}, {"sp_0": wrap(z - 1, 8)}
    xp, xm = {"sp_1": wrap(x + 1, 4)}, {"sp_1": wrap(x - 1, 4)}
    other = {"sp_2": 1 - c}
    xl, xr, xf = wrap(x - 1, 4), wrap(x + 1, 4), wrap(x + 2, 4)

    def piece(zz, xx, cols, rows=whole):
        return wv.at[zz, xx, c, rows, cols]

    def group(zz, rows=whole):
        return wv.at[zz, :, c, rows, cols_a]

    def send(view, dev, sem):
        wire.send(view, view, dev, sem)

    def arrive(view, sem):
        wire.arrive(view, sem, other)

    def a1(d, h):
        return rsem.at[d * 2 + h]

    def a1f(d):
        return rsem.at[4 + d]

    def a2(d, s):
        return rsem.at[6 + d * 4 + s - 1]

    def b1(d, s):
        return rsem.at[14 + d * 4 + s - 1]

    def b2(d, s):
        return rsem.at[22 + d * 8 + s]

    def b2f(d, s):
        return rsem.at[38 + d * 8 + s]

    def along_x(off):
        v = piece(wrap(z + off, 8), x, cols_b)
        send(v, xp, b2(0, off % 8))
        send(v, xm, b2(1, off % 8))
        send(v, other, psem)

    def start():
        send(piece(z, x, cols_b), zp, b1(0, 1))
        send(piece(z, x, cols_b), zm, b1(1, 1))
        send(piece(z, x, cols_a, half[0]), xp, a1(0, 0))
        send(piece(z, x, cols_a, half[1]), xm, a1(1, 1))
        send(piece(z, x, cols_a, half[1]), xp, a1(0, 1))
        send(piece(z, x, cols_a, half[0]), xm, a1(1, 0))
        along_x(0)

    def row_far():
        v = piece(z, xl, cols_a, half[0])
        arrive(v, a1(0, 0))
        send(v, xp, a1f(0))
        v = piece(z, xr, cols_a, half[1])
        arrive(v, a1(1, 1))
        send(v, xm, a1f(1))

    def row_done():
        arrive(piece(z, xl, cols_a, half[1]), a1(0, 1))
        arrive(piece(z, xr, cols_a, half[0]), a1(1, 0))
        arrive(piece(z, xf, cols_a, half[0]), a1f(0))
        arrive(piece(z, xf, cols_a, half[1]), a1f(1))
        send(group(z), zp, a2(0, 1))
        send(group(z), zm, a2(1, 1))
        send(group(z), other, psem)

    def z_piece(s):
        zl, zr = wrap(z - s, 8), wrap(z + s, 8)
        if s < 4:
            v = piece(zl, x, cols_b)
            arrive(v, b1(0, s))
            send(v if s < 3 else piece(zl, x, cols_b, half[0]), zp, b1(0, s + 1))
            v = piece(zr, x, cols_b)
            arrive(v, b1(1, s))
            send(v if s < 3 else piece(zr, x, cols_b, half[1]), zm, b1(1, s + 1))
            along_x(-s)
            along_x(s)
        else:
            arrive(piece(zl, x, cols_b, half[0]), b1(0, 4))
            arrive(piece(zl, x, cols_b, half[1]), b1(1, 4))
            along_x(4)

    def z_group(s):
        zl, zr = wrap(z - s, 8), wrap(z + s, 8)
        if s < 4:
            arrive(group(zl), a2(0, s))
            send(group(zl) if s < 3 else group(zl, half[0]), zp, a2(0, s + 1))
            arrive(group(zr), a2(1, s))
            send(group(zr) if s < 3 else group(zr, half[1]), zm, a2(1, s + 1))
            send(group(zl), other, psem)
            send(group(zr), other, psem)
        else:
            arrive(group(zl, half[0]), a2(0, 4))
            arrive(group(zl, half[1]), a2(1, 4))
            send(group(zl), other, psem)

    def x_piece(off):
        zz = wrap(z + off, 8)
        v = piece(zz, xl, cols_b)
        arrive(v, b2(0, off % 8))
        send(piece(zz, xl, cols_b, half[0]), xp, b2f(0, off % 8))
        send(v, other, psem)
        v = piece(zz, xr, cols_b)
        arrive(v, b2(1, off % 8))
        send(piece(zz, xr, cols_b, half[1]), xm, b2f(1, off % 8))
        send(v, other, psem)

    def x_far(off):
        zz = wrap(z + off, 8)
        arrive(piece(zz, xf, cols_b, half[0]), b2f(0, off % 8))
        arrive(piece(zz, xf, cols_b, half[1]), b2f(1, off % 8))
        send(piece(zz, xf, cols_b), other, psem)

    def finish():
        arrive(wv.at[pl.ds(0, 4)], psem)

    return [
        start,
        row_far,
        lambda: z_piece(1),
        row_done,
        lambda: x_piece(0),
        lambda: z_piece(2),
        lambda: (x_piece(-1), x_piece(1)),
        lambda: z_group(1),
        lambda: z_piece(3),
        lambda: (x_piece(-2), x_piece(2), x_far(0)),
        lambda: z_piece(4),
        lambda: z_group(2),
        lambda: (x_piece(-3), x_piece(3), x_far(1), x_far(-1)),
        lambda: (x_piece(4), x_far(2), x_far(-2)),
        lambda: z_group(3),
        lambda: (x_far(3), x_far(-3), x_far(4)),
        lambda: z_group(4),
        finish,
    ]


def thirds(v):
    high = v.astype(BF16)
    rest = v - high.astype(F32)
    mid = rest.astype(BF16)
    return high, mid, (rest - mid.astype(F32)).astype(BF16)


def dot(a, b):
    return jnp.dot(a, b, preferred_element_type=F32)


def exact_left(selector, v):
    return sum(dot(selector, part) for part in thirds(v))


def spread(v, onehot):
    return sum(dot(part, onehot) for part in thirds(v))


def silu(v):
    return v * (1.0 / (1.0 + jnp.exp(-v)))


def layer_norm(values, scales):
    centred = values - jnp.mean(values, axis=-1, keepdims=True)
    spread_of = jnp.mean(centred * centred, axis=-1, keepdims=True)
    return centred * lax.rsqrt(spread_of + EPSILON) * scales


def layer_kernel(
    resid,
    valve,
    x_in,
    b_in,
    c_in,
    deltas,
    offset,
    speed,
    fading,
    bypass,
    x_taps,
    b_taps,
    c_taps,
    cluster,
    w_mix,
    scale_one,
    w_gate,
    w_up,
    w_down,
    gate_taps,
    up_taps,
    scale_two,
    out,
    wv,
    x_rim,
    b_rim,
    c_rim,
    xs,
    bs,
    cs,
    cums,
    turned,
    ec,
    yw,
    states,
    decays,
    ends,
    row_ends,
    row_decay,
    row_pre,
    row_dpre,
    own_decay,
    z_state,
    z_decay,
    z_out,
    z_dout,
    z_acc,
    to_row,
    incoming,
    mix_out,
    mix_far,
    mix_in,
    nall,
    gu,
    ffn_out,
    ffn_far,
    ffn_in,
    send_sem,
    gather_sem,
    pair_sem,
    rim_sem,
    row_sem,
    z_sem,
    back_sem,
    mix_sem,
    all_sem,
    ffn_sem,
):
    ids = tuple(lax.axis_index(name) for name in SP_TP)
    z, x, c, y = ids
    rank = z * 8 + x * 2 + c
    place = x * 2 + c
    wire = Wire(send_sem)

    def rank_dev(r, tp=None):
        dev = {"sp_0": lax.div(r, 8), "sp_1": lax.div(lax.rem(r, 8), 2), "sp_2": lax.rem(r, 2)}
        if tp is not None:
            dev["tp"] = tp
        return dev

    def row_dev(p):
        return {"sp_1": lax.div(p, 2), "sp_2": lax.rem(p, 2)}

    after, before = wrap(rank + 1, 64), wrap(rank - 1, 64)
    right, left = {"tp": wrap(y + 1, 4)}, {"tp": wrap(y - 1, 4)}

    sem = pltpu.get_barrier_semaphore()
    greeted = [{"sp_0": wrap(z + k, 8)} for k in range(1, 8)]
    greeted += [row_dev(wrap(place + k, 8)) for k in range(1, 8)]
    greeted += [right, left]
    greeted += [rank_dev(before, k) for k in range(4)]
    for dev in greeted:
        pl.semaphore_signal(sem, inc=1, device_id=dev, device_id_type=MESH)

    ident = (
        lax.broadcasted_iota(jnp.int32, (32, 32), 0) == lax.broadcasted_iota(jnp.int32, (32, 32), 1)
    ).astype(BF16)
    wv[z, x, c, :, 0:FF] = w_gate[...]
    wv[z, x, c, :, FF : 2 * FF] = w_up[...]
    wv[z, x, c, :, 2 * FF :] = lax.dot_general(
        ident, w_down[...], NT, preferred_element_type=F32
    ).astype(BF16)
    pl.semaphore_wait(sem, len(greeted))

    has_next, has_last = rank < 63, rank > 0
    last = pl.ds(ROWS - 16, 16)
    for k, (src, dst) in enumerate(((x_in, x_rim), (b_in, b_rim), (c_in, c_rim))):
        wire.send(src.at[last], dst, rank_dev(after), rim_sem.at[k], when=has_next)
    gather = weight_gather(wire, wv, gather_sem, pair_sem, ids)
    gather[0]()

    rows_at = lax.broadcasted_iota(jnp.int32, (BLOCK, BLOCK), 0)
    cols_at = lax.broadcasted_iota(jnp.int32, (BLOCK, BLOCK), 1)
    causal = rows_at >= cols_at
    tril = causal.astype(BF16)
    onehot = (
        lax.broadcasted_iota(jnp.int32, (HEADS, INNER), 0)
        == lax.div(lax.broadcasted_iota(jnp.int32, (HEADS, INNER), 1), HEAD_DIM)
    ).astype(BF16)
    skip = spread(jnp.broadcast_to(bypass[...], (8, HEADS)), onehot)[0:1]
    low_lanes = lax.broadcasted_iota(jnp.int32, (BLOCK, 2 * HEAD_DIM), 1) < HEAD_DIM

    def conv_block(src, rim, taps, b):
        if b == 0:
            window = jnp.concatenate([rim[...], src[0:BLOCK]], axis=0).astype(F32)
        else:
            window = src[b * BLOCK - 16 : (b + 1) * BLOCK].astype(F32)
        weights = taps[...].astype(F32)
        total = weights[0:1] * window[13 : 13 + BLOCK]
        for k in range(1, 4):
            total = total + weights[k : k + 1] * window[13 + k : 13 + k + BLOCK]
        return silu(total)

    def local_block(b):
        span = slice(b * BLOCK, (b + 1) * BLOCK)
        x_act = conv_block(x_in, x_rim, x_taps, b).astype(BF16)
        b_act = conv_block(b_in, b_rim, b_taps, b).astype(BF16)
        xs[span] = x_act
        bs[span] = b_act
        cs[span] = conv_block(c_in, c_rim, c_taps, b).astype(BF16)
        raw = deltas[span] + offset[...]
        step = jnp.maximum(raw, 0.0) + jnp.log1p(jnp.exp(-jnp.abs(raw)))
        cum = exact_left(tril, fading[span] - speed[...] * step)
        cums[span, 0:HEADS] = cum
        cums[span, HEADS : 2 * HEADS] = step
        turned[b] = cums[span].T[0 : 2 * HEADS]
        grown = spread(jnp.exp(cum), onehot)
        ec[span] = grown
        to_end = spread(step * jnp.exp(cum[BLOCK - 1 : BLOCK] - cum), onehot)
        weighted = (x_act.astype(F32) * to_end).astype(BF16)
        states[b] = dot(b_act.astype(F32).T.astype(BF16), weighted)
        decays[b] = jnp.broadcast_to(grown[BLOCK - 1 : BLOCK], (8, INNER))

    def within_block(b):
        span = slice(b * BLOCK, (b + 1) * BLOCK)
        affinity = lax.dot_general(cs[span], bs[span], NT, preferred_element_type=F32)
        for pair in range(HEADS // 2):
            lanes = slice(pair * 128, (pair + 1) * 128)
            mixing = []
            for h in (2 * pair, 2 * pair + 1):
                between = cums[span, h : h + 1] - turned[b, h : h + 1]
                lag = jnp.exp(jnp.where(causal, between, -1e30))
                mixing.append((affinity * lag * turned[b, HEADS + h : HEADS + h + 1]).astype(BF16))
            x_pair = xs[span, lanes]
            zero = jnp.zeros_like(x_pair)
            sides = jnp.concatenate(
                [jnp.where(low_lanes, x_pair, zero), jnp.where(low_lanes, zero, x_pair)], axis=0
            )
            yw[span, lanes] = dot(jnp.concatenate(mixing, axis=1), sides) + skip[
                :, lanes
            ] * x_pair.astype(F32)

    def packed(v):
        return jnp.concatenate([v[:, k * 128 : (k + 1) * 128] for k in range(4)], axis=0)

    def unpacked(tile):
        return jnp.concatenate([tile[k : k + 1] for k in range(4)], axis=1)

    cums[...] = jnp.zeros_like(cums)
    local_block(3)
    gather[1]()
    local_block(2)
    local_block(1)

    @pl.when(has_last)
    def _():
        for k, dst in enumerate((x_rim, b_rim, c_rim)):
            wire.arrive(dst, rim_sem.at[k], rank_dev(before))

    @pl.when(jnp.logical_not(has_last))
    def _():
        for dst in (x_rim, b_rim, c_rim):
            dst[...] = jnp.zeros_like(dst)

    local_block(0)

    total = jnp.zeros((STATE, INNER), F32)
    growth = jnp.ones((1, INNER), F32)
    for b in range(BLOCKS):
        fresh, decay = states[b], decays[b, 0:1]
        states[b] = total
        decays[b] = jnp.broadcast_to(growth, (8, INNER))
        total = total * decay + fresh
        growth = growth * decay
    ends[...] = total.astype(BF16)
    own_decay[...] = jnp.zeros_like(own_decay)
    own_decay[0:4] = packed(growth)

    def sixteen(p):
        return pl.ds(pl.multiple_of(p * 16, 16), 16)

    for k in range(1, 8):
        to = wrap(place + k, 8)
        wire.send(ends.at[sixteen(to)], row_ends.at[place], row_dev(to), row_sem.at[0, k])
        wire.send(own_decay, row_decay.at[place], row_dev(to), row_sem.at[1, k])
    row_ends[place] = ends[sixteen(place), :]
    row_decay[place] = own_decay[...]
    gather[2]()
    within_block(0)
    within_block(1)
    for k in range(1, 8):
        src = wrap(place - k, 8)
        wire.arrive(row_ends.at[src], row_sem.at[0, k], row_dev(src))
        wire.arrive(row_decay.at[src], row_sem.at[1, k], row_dev(src))
    total = jnp.zeros((16, INNER), F32)
    growth = jnp.ones((1, INNER), F32)
    for q in range(8):
        decay = unpacked(row_decay[q])
        row_pre[q] = total
        row_dpre[q] = jnp.broadcast_to(growth, (8, INNER))
        total = total * decay + row_ends[q].astype(F32)
        growth = growth * decay
    z_out[...] = total.astype(BF16)
    z_dout[...] = jnp.zeros_like(z_dout)
    z_dout[0:4] = packed(growth)
    for k in range(1, 8):
        to = {"sp_0": wrap(z + k, 8)}
        wire.send(z_out, z_state.at[k], to, z_sem.at[0, k], when=z + k < 8)
        wire.send(z_dout, z_decay.at[k], to, z_sem.at[1, k], when=z + k < 8)
    gather[3]()
    within_block(2)
    within_block(3)
    z_acc[...] = jnp.zeros_like(z_acc)
    for k in range(7, 0, -1):

        @pl.when(z >= k)
        def _():
            src = {"sp_0": wrap(z - k, 8)}
            wire.arrive(z_state.at[k], z_sem.at[0, k], src)
            wire.arrive(z_decay.at[k], z_sem.at[1, k], src)
            z_acc[...] = z_acc[...] * unpacked(z_decay[k]) + z_state[k].astype(F32)

    begun = z_acc[...]
    for q in range(8):
        to_row[q] = (begun * row_dpre[q, 0:1] + row_pre[q]).astype(BF16)
    for k in range(1, 8):
        to = wrap(place + k, 8)
        wire.send(to_row.at[to], incoming.at[sixteen(place)], row_dev(to), back_sem.at[k])
    incoming[sixteen(place), :] = to_row[place]
    gather[4]()
    gather[5]()
    for k in range(1, 8):
        src = wrap(place - k, 8)
        wire.arrive(incoming.at[sixteen(src)], back_sem.at[k], row_dev(src))

    turns = [wrap(y + 2, 4), wrap(y + 1, 4), wrap(y - 1, 4), y]

    def reduce_rows(part, sent, far, got, sems, fill):
        upper, lower = pl.ds(0, 64), pl.ds(64, 64)
        part(0)
        wire.send(sent.at[0, upper], far.at[0], right, sems.at[0])
        wire.send(sent.at[0, lower], far.at[1], left, sems.at[1])
        part(1)
        wire.send(sent.at[1, lower], got.at[0, lower], right, sems.at[2])
        part(2)
        wire.send(sent.at[2, upper], got.at[1, upper], left, sems.at[3])
        fill(0)
        wire.arrive(far.at[0], sems.at[0], left)
        sent[1, 0:64] = (sent[1, 0:64].astype(F32) + far[0].astype(F32)).astype(BF16)
        wire.send(sent.at[1, upper], got.at[0, upper], right, sems.at[4])
        wire.arrive(far.at[1], sems.at[1], right)
        sent[2, 64:128] = (sent[2, 64:128].astype(F32) + far[1].astype(F32)).astype(BF16)
        wire.send(sent.at[2, lower], got.at[1, lower], left, sems.at[5])
        part(3)
        fill(1)
        wire.arrive(got.at[0, lower], sems.at[2], left)
        wire.arrive(got.at[1, upper], sems.at[3], right)
        wire.arrive(got.at[0, upper], sems.at[4], left)
        wire.arrive(got.at[1, lower], sems.at[5], right)
        return sent[3].astype(F32) + got[0].astype(F32) + got[1].astype(F32)

    def mix_part(k):
        t = turns[k]
        span = pl.ds(pl.multiple_of(t * BLOCK, BLOCK), BLOCK)
        begin = states[t] + incoming[...].astype(F32) * decays[t, 0:1]
        gated = yw[span, :] + ec[span, :] * dot(cs[span, :], begin.astype(BF16))
        gated = gated * silu(valve[span, :].astype(F32))
        gated = gated * lax.rsqrt(jnp.mean(gated * gated, axis=-1, keepdims=True) + EPSILON)
        y_norm = (gated * cluster[...]).astype(BF16)
        for j in range(4):
            lanes = slice(j * 512, (j + 1) * 512)
            mix_out[k, :, lanes] = dot(y_norm, w_mix[:, lanes]).astype(BF16)

    def mix_fill(stage):
        for event in (gather[6:8], gather[8:11])[stage]:
            event()

    mixer = reduce_rows(mix_part, mix_out, mix_far, mix_in, mix_sem, mix_fill)
    normed = layer_norm(ALPHA * resid[...].astype(F32) + mixer, scale_one[...]).astype(BF16)

    def chunk(t):
        return pl.ds(pl.multiple_of(16 + t * BLOCK, 16), BLOCK)

    def chunk_half(t, h):
        return pl.ds(pl.multiple_of(16 + t * BLOCK + h * 64, 16), 64)

    nall[chunk(y), :] = normed
    for h in range(2):
        for dev, half_of in ((right, h), (left, 1 - h)):
            v = nall.at[chunk_half(y, half_of)]
            wire.send(v, v, dev, all_sem.at[0 if dev is right else 1, half_of])
    for k in range(4):
        wire.send(
            nall.at[pl.ds(pl.multiple_of(y * BLOCK + BLOCK, 16), 16)],
            nall.at[pl.ds(0, 16)],
            rank_dev(after, k),
            all_sem.at[3, 0],
            when=jnp.logical_and(has_next, y == 3),
        )

    def project(span):
        rows = nall[span, :]

        def tile(j, carry):
            lanes = pl.ds(pl.multiple_of(j * 256, 256), 256)
            gu[span, lanes] = (
                dot(rows, wv[:, :, :, :, lanes].reshape(D, 256)).astype(BF16).astype(F32)
            )
            return carry

        lax.fori_loop(0, 11, tile, 0)

    far_t, right_t, left_t = turns[0], turns[1], turns[2]
    v = nall.at[chunk_half(left_t, 0)]
    wire.arrive(v, all_sem.at[0, 0], left)
    wire.send(v, v, right, all_sem.at[2, 0])
    v = nall.at[chunk_half(right_t, 1)]
    wire.arrive(v, all_sem.at[1, 1], right)
    wire.send(v, v, left, all_sem.at[2, 1])
    for event in gather[11:]:
        event()
    project(chunk(y))

    @pl.when(has_last)
    def _():
        wire.arrive(nall.at[pl.ds(0, 16)], all_sem.at[3, 0], rank_dev(before, 3))

    @pl.when(jnp.logical_not(has_last))
    def _():
        nall[0:16] = jnp.zeros((16, D), BF16)

    project(pl.ds(0, 16))
    wire.arrive(nall.at[chunk_half(left_t, 1)], all_sem.at[0, 1], left)
    project(chunk(left_t))
    wire.arrive(nall.at[chunk_half(right_t, 0)], all_sem.at[1, 0], right)
    project(chunk(right_t))
    wire.arrive(nall.at[chunk_half(far_t, 0)], all_sem.at[2, 0], left)
    wire.arrive(nall.at[chunk_half(far_t, 1)], all_sem.at[2, 1], right)
    project(chunk(far_t))

    def conv_gu(t, lanes, taps, tap_lanes):
        window = gu[pl.ds(pl.multiple_of(t * BLOCK + 8, 8), BLOCK + 8), lanes]
        weights = taps[:, tap_lanes].astype(F32)
        total = weights[0:1] * window[6 : 6 + BLOCK]
        for k in range(1, 3):
            total = total + weights[k : k + 1] * window[6 + k : 6 + k + BLOCK]
        return total

    def ffn_part(k):
        t = turns[k]
        pieces = []
        for j in range(11):
            lanes = slice(j * 128, (j + 1) * 128)
            shifted_lanes = slice(FF + j * 128, FF + (j + 1) * 128)
            gate = conv_gu(t, lanes, gate_taps, lanes)
            pieces.append((silu(gate) * conv_gu(t, shifted_lanes, up_taps, lanes)).astype(BF16))
        hidden = jnp.concatenate(pieces, axis=1)
        for j in range(4):
            w = wv[2 * j : 2 * j + 2, :, :, :, 2 * FF :].reshape(512, FF)
            ffn_out[k, :, j * 512 : (j + 1) * 512] = lax.dot_general(
                hidden, w, NT, preferred_element_type=F32
            ).astype(BF16)

    channel = reduce_rows(ffn_part, ffn_out, ffn_far, ffn_in, ffn_sem, lambda stage: None)
    out[...] = layer_norm(
        ALPHA * nall[chunk(y), :].astype(F32) + channel, scale_two[...]
    ).astype(BF16)
    wire.finish()


def shards(*arrays):
    arrays = [a.reshape(1, -1) if a.ndim == 1 else a for a in arrays]
    dma = pltpu.SemaphoreType.DMA
    scratch = [
        pltpu.VMEM((8, 4, 2, 32, COLS), BF16),
        pltpu.VMEM((16, INNER), BF16),
        pltpu.VMEM((16, STATE), BF16),
        pltpu.VMEM((16, STATE), BF16),
        pltpu.VMEM((ROWS, INNER), BF16),
        pltpu.VMEM((ROWS, STATE), BF16),
        pltpu.VMEM((ROWS, STATE), BF16),
        pltpu.VMEM((ROWS, 128), F32),
        pltpu.VMEM((BLOCKS, 2 * HEADS, BLOCK), F32),
        pltpu.VMEM((ROWS, INNER), F32),
        pltpu.VMEM((ROWS, INNER), F32),
        pltpu.VMEM((BLOCKS, STATE, INNER), F32),
        pltpu.VMEM((BLOCKS, 8, INNER), F32),
        pltpu.VMEM((STATE, INNER), BF16),
        pltpu.VMEM((8, 16, INNER), BF16),
        pltpu.VMEM((8, 8, 128), F32),
        pltpu.VMEM((8, 16, INNER), F32),
        pltpu.VMEM((8, 8, INNER), F32),
        pltpu.VMEM((8, 128), F32),
        pltpu.VMEM((8, 16, INNER), BF16),
        pltpu.VMEM((8, 8, 128), F32),
        pltpu.VMEM((16, INNER), BF16),
        pltpu.VMEM((8, 128), F32),
        pltpu.VMEM((16, INNER), F32),
        pltpu.VMEM((8, 16, INNER), BF16),
        pltpu.VMEM((STATE, INNER), BF16),
        pltpu.VMEM((4, BLOCK, D), BF16),
        pltpu.VMEM((2, 64, D), BF16),
        pltpu.VMEM((2, BLOCK, D), BF16),
        pltpu.VMEM((ROWS + 16, D), BF16),
        pltpu.VMEM((ROWS + 16, 2 * FF), F32),
        pltpu.VMEM((4, BLOCK, D), BF16),
        pltpu.VMEM((2, 64, D), BF16),
        pltpu.VMEM((2, BLOCK, D), BF16),
        dma((180,)),
        dma((54,)),
        dma,
        dma((3,)),
        dma((2, 8)),
        dma((2, 8)),
        dma((8,)),
        dma((6,)),
        dma((4, 2)),
        dma((6,)),
    ]
    return pl.pallas_call(
        layer_kernel,
        out_shape=jax.ShapeDtypeStruct((BLOCK, D), BF16),
        in_specs=[pl.BlockSpec(memory_space=pltpu.VMEM)] * len(arrays),
        out_specs=pl.BlockSpec(memory_space=pltpu.VMEM),
        scratch_shapes=scratch,
        compiler_params=pltpu.CompilerParams(
            collective_id=0, has_side_effects=True, vmem_limit_bytes=67043328
        ),
    )(*arrays)


def solution(mesh):
    split = Mesh(mesh.devices.reshape(8, 4, 2, mesh.shape["tp"]), ("sp_0", "sp_1", "sp_2", "tp"))
    in_specs = (
        P(SP_TP, None),
        P(SP, "tp"),
        P(SP, "tp"),
        P(SP, "tp"),
        P(SP, "tp"),
        P(SP, "tp"),
        P("tp"),
        P("tp"),
        P(SP, "tp"),
        P("tp"),
        P(None, "tp"),
        P(None, "tp"),
        P(None, "tp"),
        P("tp"),
        P("tp", None),
        P(),
        P(SP, "tp"),
        P(SP, "tp"),
        P("tp", SP),
        P(None, "tp"),
        P(None, "tp"),
        P(),
    )
    out_specs = P(SP_TP, None)
    return jax.shard_map(
        shards, mesh=split, in_specs=in_specs, out_specs=out_specs, check_vma=False
    )
```

```python
import jax
import jax.numpy as jnp
from jax import lax
from jax.experimental import pallas as pl
from jax.experimental.pallas import tpu as pltpu
from jax.sharding import Mesh
from jax.sharding import PartitionSpec as P

HEADS = 8
HEAD_DIM = 64
STATE = 128
BLOCK = 128
BLOCKS = 4
ROWS = BLOCK * BLOCKS
INNER = 512
D = 2048
FF = 1408
COLS = 3 * FF
NA = 1792
EPSILON = 1e-05
ALPHA = 2.0**0.25
SP = ("sp_0", "sp_1", "sp_2")
SP_TP = ("sp_0", "sp_1", "sp_2", "tp")
MESH = pl.DeviceIdType.MESH
F32 = jnp.float32
BF16 = jnp.bfloat16
NT = (((1,), (1,)), ((), ()))


def wrap(value, count):
    return lax.rem(value + 2 * count, count)


class Marks:
    def __init__(self):
        self.scope = None

    def __call__(self, name):
        self.end()
        self.scope = jax.named_scope(name)
        self.scope.__enter__()

    def end(self):
        if self.scope is not None:
            self.scope.__exit__(None, None, None)
            self.scope = None


class Wire:
    def __init__(self, send_sem):
        self.send_sem = send_sem
        self.count = 0
        self.waits = []

    def send(self, src, dst, dev, recv_sem, when=None):
        copy = pltpu.make_async_remote_copy(
            src_ref=src,
            dst_ref=dst,
            send_sem=self.send_sem.at[self.count],
            recv_sem=recv_sem,
            device_id=dev,
            device_id_type=MESH,
        )
        self.count += 1
        if when is None:
            copy.start()
        else:
            pl.when(when)(copy.start)
        self.waits.append((copy, when))

    def arrive(self, dst, recv_sem, dev):
        pltpu.make_async_remote_copy(
            src_ref=dst,
            dst_ref=dst,
            send_sem=self.send_sem.at[0],
            recv_sem=recv_sem,
            device_id=dev,
            device_id_type=MESH,
        ).wait_recv()

    def finish(self):
        for copy, when in self.waits:
            if when is None:
                copy.wait_send()
            else:
                pl.when(when)(copy.wait_send)


def weight_gather(wire, wv, rsem, psem, ids, mark):
    z, x, c, _ = ids
    cols_a, cols_b = pl.ds(0, NA), pl.ds(NA, COLS - NA)
    half, whole = (pl.ds(0, 16), pl.ds(16, 16)), pl.ds(0, 32)
    zp, zm = {"sp_0": wrap(z + 1, 8)}, {"sp_0": wrap(z - 1, 8)}
    xp, xm = {"sp_1": wrap(x + 1, 4)}, {"sp_1": wrap(x - 1, 4)}
    other = {"sp_2": 1 - c}
    xl, xr, xf = wrap(x - 1, 4), wrap(x + 1, 4), wrap(x + 2, 4)

    def pair(off):
        return psem.at[off % 8]

    def piece(zz, xx, cols, rows=whole):
        return wv.at[zz, xx, c, rows, cols]

    def group(zz, rows=whole):
        return wv.at[zz, :, c, rows, cols_a]

    def send(view, dev, sem):
        wire.send(view, view, dev, sem)

    def arrive(view, sem):
        wire.arrive(view, sem, other)

    def a1(d, h):
        return rsem.at[d * 2 + h]

    def a1f(d):
        return rsem.at[4 + d]

    def b1(d, s):
        return rsem.at[14 + d * 4 + s - 1]

    def b2(d, s):
        return rsem.at[22 + d * 8 + s]

    def b2f(d, s):
        return rsem.at[38 + d * 8 + s]

    def a2(d, s, k):
        return rsem.at[54 + d * 16 + (s - 1) * 4 + k]

    columns = (x, xl, xr, xf)

    def x_send(off):
        v = piece(wrap(z + off, 8), x, cols_b)
        send(v, xp, b2(0, off % 8))
        send(v, xm, b2(1, off % 8))

    def start():
        send(piece(z, x, cols_a, half[0]), xp, a1(0, 0))
        send(piece(z, x, cols_a, half[1]), xm, a1(1, 1))
        send(piece(z, x, cols_a, half[1]), xp, a1(0, 1))
        send(piece(z, x, cols_a, half[0]), xm, a1(1, 0))
        send(piece(z, x, cols_b), zp, b1(0, 1))
        send(piece(z, x, cols_b), zm, b1(1, 1))
        send(piece(z, x, cols_a), zp, a2(0, 1, 0))
        send(piece(z, x, cols_a), zm, a2(1, 1, 0))
        send(piece(z, x, cols_b), other, pair(0))

    def row_far():
        v = piece(z, xl, cols_a, half[0])
        arrive(v, a1(0, 0))
        send(v, xp, a1f(0))
        v = piece(z, xr, cols_a, half[1])
        arrive(v, a1(1, 1))
        send(v, xm, a1f(1))

    def row_done():
        arrive(piece(z, xl, cols_a, half[1]), a1(0, 1))
        arrive(piece(z, xr, cols_a, half[0]), a1(1, 0))
        arrive(piece(z, xf, cols_a, half[0]), a1f(0))
        arrive(piece(z, xf, cols_a, half[1]), a1f(1))
        for k in range(1, 4):
            send(piece(z, columns[k], cols_a), zp, a2(0, 1, k))
            send(piece(z, columns[k], cols_a), zm, a2(1, 1, k))
        send(group(z), other, pair(0))

    def z_piece(s):
        zl, zr = wrap(z - s, 8), wrap(z + s, 8)
        if s < 4:
            v = piece(zl, x, cols_b)
            arrive(v, b1(0, s))
            send(v if s < 3 else piece(zl, x, cols_b, half[0]), zp, b1(0, s + 1))
            send(v, other, pair(-s))
            v = piece(zr, x, cols_b)
            arrive(v, b1(1, s))
            send(v if s < 3 else piece(zr, x, cols_b, half[1]), zm, b1(1, s + 1))
            send(v, other, pair(s))
        else:
            arrive(piece(zl, x, cols_b, half[0]), b1(0, 4))
            arrive(piece(zl, x, cols_b, half[1]), b1(1, 4))
            send(piece(zl, x, cols_b), other, pair(4))

    def z_group(s, *which):
        zl, zr = wrap(z - s, 8), wrap(z + s, 8)
        for k in which:
            if s < 4:
                v = piece(zl, columns[k], cols_a)
                arrive(v, a2(0, s, k))
                send(v if s < 3 else piece(zl, columns[k], cols_a, half[0]), zp, a2(0, s + 1, k))
                v = piece(zr, columns[k], cols_a)
                arrive(v, a2(1, s, k))
                send(v if s < 3 else piece(zr, columns[k], cols_a, half[1]), zm, a2(1, s + 1, k))
            else:
                arrive(piece(zl, columns[k], cols_a, half[0]), a2(0, 4, k))
                arrive(piece(zl, columns[k], cols_a, half[1]), a2(1, 4, k))
        if 3 in which:
            send(group(zl), other, pair(-s))
            if s < 4:
                send(group(zr), other, pair(s))

    def x_piece(off):
        zz = wrap(z + off, 8)
        v = piece(zz, xl, cols_b)
        arrive(v, b2(0, off % 8))
        send(piece(zz, xl, cols_b, half[0]), xp, b2f(0, off % 8))
        send(v, other, pair(off))
        v = piece(zz, xr, cols_b)
        arrive(v, b2(1, off % 8))
        send(piece(zz, xr, cols_b, half[1]), xm, b2f(1, off % 8))
        send(v, other, pair(off))

    def x_far(off):
        zz = wrap(z + off, 8)
        arrive(piece(zz, xf, cols_b, half[0]), b2f(0, off % 8))
        arrive(piece(zz, xf, cols_b, half[1]), b2f(1, off % 8))
        send(piece(zz, xf, cols_b), other, pair(off))

    def pair_done(off):
        arrive(wv.at[wrap(z + off, 8), :, 1 - c], pair(off))

    steps = {
        "start": start,
        "row_far": row_far,
        "row_done": row_done,
        "z_piece": z_piece,
        "z_group": z_group,
        "x_send": x_send,
        "x_piece": x_piece,
        "x_far": x_far,
        "pair_done": pair_done,
    }

    def run(*plan):
        for name, *at in plan:
            mark("g_" + name + "".join(str(k) for k in at))
            steps[name](*at)

    return run


def thirds(v):
    high = v.astype(BF16)
    rest = v - high.astype(F32)
    mid = rest.astype(BF16)
    return high, mid, (rest - mid.astype(F32)).astype(BF16)


def dot(a, b):
    return jnp.dot(a, b, preferred_element_type=F32)


def spread(v, onehot):
    return sum(dot(part, onehot) for part in thirds(v))


def silu(v):
    return v * (1.0 / (1.0 + jnp.exp(-v)))


def layer_norm(values, scales):
    centred = values - jnp.mean(values, axis=-1, keepdims=True)
    spread_of = jnp.mean(centred * centred, axis=-1, keepdims=True)
    return centred * lax.rsqrt(spread_of + EPSILON) * scales


LOADED = (
    "resid",
    "valve",
    "x_in",
    "b_in",
    "c_in",
    "deltas",
    "offset",
    "speed",
    "fading",
    "bypass",
    "x_taps",
    "b_taps",
    "c_taps",
    "cluster",
    "w_mix",
    "scale_one",
    "gate_taps",
    "up_taps",
    "scale_two",
)


EARLY = LOADED[2:13]


def layer_kernel(*refs):
    sources, out, refs = refs[:22], refs[22], refs[23:]
    loads, refs = refs[:19], refs[19:]
    (
        resid,
        valve,
        x_in,
        b_in,
        c_in,
        deltas,
        offset,
        speed,
        fading,
        bypass,
        x_taps,
        b_taps,
        c_taps,
        cluster,
        w_mix,
        scale_one,
        gate_taps,
        up_taps,
        scale_two,
    ) = loads
    (
        wv,
        load_sem,
        x_rim,
        b_rim,
        c_rim,
        xs,
        bs,
        cs,
        cums,
        turned,
        ec,
        yw,
        states,
        decays,
        ends,
        row_ends,
        row_decay,
        row_pre,
        row_dpre,
        own_decay,
        z_state,
        z_decay,
        z_out,
        z_dout,
        z_acc,
        to_row,
        incoming,
        mix_out,
        mix_far,
        mix_in,
        nall,
        gu,
        ffn_out,
        ffn_far,
        ffn_in,
        send_sem,
        gather_sem,
        pair_sem,
        rim_sem,
        row_sem,
        z_sem,
        back_sem,
        mix_sem,
        all_sem,
        ffn_sem,
    ) = refs
    ids = tuple(lax.axis_index(name) for name in SP_TP)
    z, x, c, y = ids
    rank = z * 8 + x * 2 + c
    place = x * 2 + c
    wire = Wire(send_sem)

    def rank_dev(r, tp=None):
        dev = {"sp_0": lax.div(r, 8), "sp_1": lax.div(lax.rem(r, 8), 2), "sp_2": lax.rem(r, 2)}
        if tp is not None:
            dev["tp"] = tp
        return dev

    def row_dev(p):
        return {"sp_1": lax.div(p, 2), "sp_2": lax.rem(p, 2)}

    after, before = wrap(rank + 1, 64), wrap(rank - 1, 64)
    right, left = {"tp": wrap(y + 1, 4)}, {"tp": wrap(y - 1, 4)}

    mark = Marks()
    mark("barrier")
    sem = pltpu.get_barrier_semaphore()
    greeted = [{"sp_0": wrap(z + k, 8)} for k in range(1, 8)]
    greeted += [row_dev(wrap(place + k, 8)) for k in range(1, 8)]
    greeted += [right, left]
    greeted += [rank_dev(before, k) for k in range(4)]
    for dev in greeted:
        pl.semaphore_signal(sem, inc=1, device_id=dev, device_id_type=MESH)

    sources, shards_here = sources[:16] + sources[19:], sources[16:19]
    copies = [
        pltpu.make_async_copy(src, wv.at[z, x, c, :, pl.ds(k * FF, FF)], load_sem.at[19 + k])
        for k, src in enumerate(shards_here)
    ]
    order = sorted(range(19), key=lambda k: LOADED[k] not in EARLY)
    copies += [pltpu.make_async_copy(sources[k], loads[k], load_sem.at[k]) for k in order]
    for copy in copies:
        copy.start()
    for copy in copies[: 3 + len(EARLY)]:
        copy.wait()
    pl.semaphore_wait(sem, len(greeted))

    has_next, has_last = rank < 63, rank > 0
    last = pl.ds(ROWS - 16, 16)
    for k, (src, dst) in enumerate(((x_in, x_rim), (b_in, b_rim), (c_in, c_rim))):
        wire.send(src.at[last], dst, rank_dev(after), rim_sem.at[k], when=has_next)
    gather = weight_gather(wire, wv, gather_sem, pair_sem, ids, mark)
    gather(("start",))

    rows_at = lax.broadcasted_iota(jnp.int32, (BLOCK, BLOCK), 0)
    cols_at = lax.broadcasted_iota(jnp.int32, (BLOCK, BLOCK), 1)
    causal = rows_at >= cols_at
    triu = (rows_at <= cols_at).astype(BF16)
    onehot = (
        lax.broadcasted_iota(jnp.int32, (HEADS, INNER), 0)
        == lax.div(lax.broadcasted_iota(jnp.int32, (HEADS, INNER), 1), HEAD_DIM)
    ).astype(BF16)
    eye = lax.broadcasted_iota(jnp.int32, (HEADS, HEADS), 0) == lax.broadcasted_iota(
        jnp.int32, (HEADS, HEADS), 1
    )

    def turned_up(v):
        return jnp.sum(
            jnp.where(eye, jnp.broadcast_to(v[...], (HEADS, HEADS)), 0.0), axis=1, keepdims=True
        )

    offset_col, speed_col = turned_up(offset), turned_up(speed)
    skip = spread(jnp.broadcast_to(bypass[...], (8, HEADS)), onehot)[0:1]
    low_lanes = lax.broadcasted_iota(jnp.int32, (BLOCK, 2 * HEAD_DIM), 1) < HEAD_DIM

    def conv_block(src, rim, taps, b):
        if b == 0:
            window = jnp.concatenate([rim[...], src[0:BLOCK]], axis=0).astype(F32)
        else:
            window = src[b * BLOCK - 16 : (b + 1) * BLOCK].astype(F32)
        weights = taps[...].astype(F32)
        total = weights[0:1] * window[13 : 13 + BLOCK]
        for k in range(1, 4):
            total = total + weights[k : k + 1] * window[13 + k : 13 + k + BLOCK]
        return silu(total)

    def local_block(b):
        span = slice(b * BLOCK, (b + 1) * BLOCK)
        x_act = conv_block(x_in, x_rim, x_taps, b).astype(BF16)
        b_act = conv_block(b_in, b_rim, b_taps, b).astype(BF16)
        xs[span] = x_act
        bs[span] = b_act
        cs[span] = conv_block(c_in, c_rim, c_taps, b).astype(BF16)
        raw = deltas[:, span] + offset_col
        step_rows = jnp.maximum(raw, 0.0) + jnp.log1p(jnp.exp(-jnp.abs(raw)))
        cum_rows = spread(fading[:, span] - speed_col * step_rows, triu)
        both = jnp.concatenate([cum_rows, step_rows], axis=0)
        turned[b] = both
        both = jnp.concatenate([both, jnp.zeros((112, BLOCK), F32)], axis=0).T
        cums[span] = both
        cum, step = both[:, 0:HEADS], both[:, HEADS : 2 * HEADS]
        grown = spread(jnp.exp(cum), onehot)
        ec[span] = grown
        to_end = spread(step * jnp.exp(cum[BLOCK - 1 : BLOCK] - cum), onehot)
        weighted = (x_act.astype(F32) * to_end).astype(BF16)
        states[b] = dot(b_act.astype(F32).T.astype(BF16), weighted)
        decays[b] = jnp.broadcast_to(grown[BLOCK - 1 : BLOCK], (8, INNER))

    def within_block(b):
        span = slice(b * BLOCK, (b + 1) * BLOCK)
        affinity = lax.dot_general(cs[span], bs[span], NT, preferred_element_type=F32)
        for pair in range(HEADS // 2):
            lanes = slice(pair * 128, (pair + 1) * 128)
            mixing = []
            for h in (2 * pair, 2 * pair + 1):
                between = cums[span, h : h + 1] - turned[b, h : h + 1]
                lag = jnp.exp(jnp.where(causal, between, -1e30))
                mixing.append((affinity * lag * turned[b, HEADS + h : HEADS + h + 1]).astype(BF16))
            x_pair = xs[span, lanes]
            zero = jnp.zeros_like(x_pair)
            sides = jnp.concatenate(
                [jnp.where(low_lanes, x_pair, zero), jnp.where(low_lanes, zero, x_pair)], axis=0
            )
            yw[span, lanes] = dot(jnp.concatenate(mixing, axis=1), sides) + skip[
                :, lanes
            ] * x_pair.astype(F32)

    def packed(v):
        return jnp.concatenate([v[:, k * 128 : (k + 1) * 128] for k in range(4)], axis=0)

    def unpacked(tile):
        return jnp.concatenate([tile[k : k + 1] for k in range(4)], axis=1)

    mark("local3")
    local_block(3)
    mark("local2")
    local_block(2)
    local_block(1)
    gather(("row_far",))
    mark("rim_wait")

    @pl.when(has_last)
    def _():
        for k, dst in enumerate((x_rim, b_rim, c_rim)):
            wire.arrive(dst, rim_sem.at[k], rank_dev(before))

    @pl.when(jnp.logical_not(has_last))
    def _():
        for dst in (x_rim, b_rim, c_rim):
            dst[...] = jnp.zeros_like(dst)

    mark("local0")
    local_block(0)
    mark("ends")

    total = jnp.zeros((STATE, INNER), F32)
    growth = jnp.ones((1, INNER), F32)
    for b in range(BLOCKS):
        fresh, decay = states[b], decays[b, 0:1]
        states[b] = total
        decays[b] = jnp.broadcast_to(growth, (8, INNER))
        total = total * decay + fresh
        growth = growth * decay
    ends[...] = total.astype(BF16)
    own_decay[...] = packed(growth)

    def sixteen(p):
        return pl.ds(pl.multiple_of(p * 16, 16), 16)

    for k in range(1, 8):
        to = wrap(place + k, 8)
        wire.send(ends.at[sixteen(to)], row_ends.at[place], row_dev(to), row_sem.at[0, k])
        wire.send(own_decay, row_decay.at[place], row_dev(to), row_sem.at[1, k])
    row_ends[place] = ends[sixteen(place), :]
    row_decay[place] = own_decay[...]
    gather(("x_send", 0), ("z_piece", 1))
    mark("within01")
    within_block(0)
    within_block(1)
    mark("row_wait")
    for k in range(1, 8):
        src = wrap(place - k, 8)
        wire.arrive(row_ends.at[src], row_sem.at[0, k], row_dev(src))
        wire.arrive(row_decay.at[src], row_sem.at[1, k], row_dev(src))
    mark("row_fold")
    total = jnp.zeros((16, INNER), F32)
    growth = jnp.ones((1, INNER), F32)
    for q in range(8):
        decay = unpacked(row_decay[q])
        row_pre[q] = total
        row_dpre[q] = jnp.broadcast_to(growth, (8, INNER))
        total = total * decay + row_ends[q].astype(F32)
        growth = growth * decay
    z_out[...] = total.astype(BF16)
    z_dout[...] = packed(growth)
    for k in range(1, 8):
        to = {"sp_0": wrap(z + k, 8)}
        wire.send(z_out, z_state.at[k], to, z_sem.at[0, k], when=z + k < 8)
        wire.send(z_dout, z_decay.at[k], to, z_sem.at[1, k], when=z + k < 8)
    gather(("row_done",))
    mark("within23")
    within_block(2)
    within_block(3)
    mark("z_wait")
    z_acc[...] = jnp.zeros_like(z_acc)
    for k in range(7, 0, -1):

        @pl.when(z >= k)
        def _():
            src = {"sp_0": wrap(z - k, 8)}
            wire.arrive(z_state.at[k], z_sem.at[0, k], src)
            wire.arrive(z_decay.at[k], z_sem.at[1, k], src)
            z_acc[...] = z_acc[...] * unpacked(z_decay[k]) + z_state[k].astype(F32)

    mark("z_fold")
    begun = z_acc[...]
    for q in range(8):
        to_row[q] = (begun * row_dpre[q, 0:1] + row_pre[q]).astype(BF16)
    for k in range(1, 8):
        to = wrap(place + k, 8)
        wire.send(to_row.at[to], incoming.at[sixteen(place)], row_dev(to), back_sem.at[k])
    incoming[sixteen(place), :] = to_row[place]
    gather(("x_send", -1), ("x_send", 1), ("x_piece", 0), ("z_piece", 2))
    mark("back_wait")
    for k in range(1, 8):
        src = wrap(place - k, 8)
        wire.arrive(incoming.at[sixteen(src)], back_sem.at[k], row_dev(src))

    for copy in copies[3 + len(EARLY) :]:
        copy.wait()
    turns = [wrap(y + 2, 4), wrap(y + 1, 4), wrap(y - 1, 4), y]

    def reduce_rows(part, sent, far, got, sems, fill, name):
        upper, lower = pl.ds(0, 64), pl.ds(64, 64)
        tiles = [pl.ds(j * 512, 512) for j in range(4)]
        mark(name + "_part0")
        tile = part(0)
        for j, lanes in enumerate(tiles):
            tile(j)
            wire.send(sent.at[0, upper, lanes], far.at[0, :, lanes], right, sems.at[j])
            wire.send(sent.at[0, lower, lanes], far.at[1, :, lanes], left, sems.at[4 + j])
        mark(name + "_part1")
        tile = part(1)
        for j in range(4):
            tile(j)
        wire.send(sent.at[1, lower], got.at[0, lower], right, sems.at[8])
        mark(name + "_part2")
        tile = part(2)
        for j in range(4):
            tile(j)
        wire.send(sent.at[2, upper], got.at[1, upper], left, sems.at[9])
        fill(0)
        mark(name + "_far_wait")
        for j, lanes in enumerate(tiles):
            at = slice(j * 512, (j + 1) * 512)
            wire.arrive(far.at[0, :, lanes], sems.at[j], left)
            sent[1, 0:64, at] = (sent[1, 0:64, at].astype(F32) + far[0, :, at].astype(F32)).astype(
                BF16
            )
            wire.send(sent.at[1, upper, lanes], got.at[0, upper, lanes], right, sems.at[10 + j])
            wire.arrive(far.at[1, :, lanes], sems.at[4 + j], right)
            sent[2, 64:, at] = (sent[2, 64:, at].astype(F32) + far[1, :, at].astype(F32)).astype(
                BF16
            )
            wire.send(sent.at[2, lower, lanes], got.at[1, lower, lanes], left, sems.at[14 + j])
        fill(1)
        mark(name + "_part3")
        tile = part(3)
        for j in range(4):
            tile(j)
        fill(2)
        mark(name + "_wait")
        wire.arrive(got.at[0, lower], sems.at[8], left)
        wire.arrive(got.at[1, upper], sems.at[9], right)
        for j, lanes in enumerate(tiles):
            wire.arrive(got.at[0, upper, lanes], sems.at[10 + j], left)
            wire.arrive(got.at[1, lower, lanes], sems.at[14 + j], right)
        return sent[3].astype(F32) + got[0].astype(F32) + got[1].astype(F32)

    def mix_part(k):
        t = turns[k]
        span = pl.ds(pl.multiple_of(t * BLOCK, BLOCK), BLOCK)
        begin = states[t] + incoming[...].astype(F32) * decays[t, 0:1]
        gated = yw[span, :] + ec[span, :] * dot(cs[span, :], begin.astype(BF16))
        gated = gated * silu(valve[span, :].astype(F32))
        gated = gated * lax.rsqrt(jnp.mean(gated * gated, axis=-1, keepdims=True) + EPSILON)
        y_norm = (gated * cluster[...]).astype(BF16)

        def tile(j):
            lanes = slice(j * 512, (j + 1) * 512)
            mix_out[k, :, lanes] = dot(y_norm, w_mix[:, lanes]).astype(BF16)

        return tile

    def mix_fill(stage):
        if stage == 0:
            gather(("x_send", -2), ("x_send", 2), ("z_group", 1, 0, 1), ("x_piece", -1), ("z_group", 1, 2, 3))
        elif stage == 1:
            gather(("z_piece", 3), ("x_piece", 1), ("x_send", -3), ("x_send", 3))
        else:
            gather(("x_piece", -2), ("x_piece", 2), ("x_far", 0))
            gather(("z_group", 2, 0, 1), ("z_piece", 4), ("z_group", 2, 2, 3), ("x_send", 4), ("x_far", -1), ("x_far", 1))

    mixer = reduce_rows(mix_part, mix_out, mix_far, mix_in, mix_sem, mix_fill, "mix")
    mark("norm_one")
    normed = layer_norm(ALPHA * resid[...].astype(F32) + mixer, scale_one[...]).astype(BF16)

    def chunk(t):
        return pl.ds(pl.multiple_of(16 + t * BLOCK, 16), BLOCK)

    def chunk_half(t, h):
        return pl.ds(pl.multiple_of(16 + t * BLOCK + h * 64, 16), 64)

    nall[chunk(y), :] = normed
    mark("all_send")
    for h in range(2):
        for dev, half_of in ((right, h), (left, 1 - h)):
            v = nall.at[chunk_half(y, half_of)]
            wire.send(v, v, dev, all_sem.at[0 if dev is right else 1, half_of])
    for k in range(4):
        wire.send(
            nall.at[pl.ds(pl.multiple_of(y * BLOCK + BLOCK, 16), 16)],
            nall.at[pl.ds(0, 16)],
            rank_dev(after, k),
            all_sem.at[3, 0],
            when=jnp.logical_and(has_next, y == 3),
        )

    def project(spans, offs, first, last_of):
        zs = [wrap(z + off, 8) for off in offs]
        deep = [pl.ds(pl.multiple_of(zz * 256, 256), 256) for zz in zs]
        rows = jnp.concatenate(
            [jnp.concatenate([nall[span, k] for k in deep], axis=1) for span in spans], axis=0
        )

        for j in range(11):
            lanes = slice(j * 256, (j + 1) * 256)
            weights = [wv[zz, :, :, :, lanes].reshape(256, 256) for zz in zs]
            got = dot(rows, jnp.concatenate(weights, axis=0))
            at = 0
            for span in spans:
                mine = got[at : at + span.size]
                at += span.size
                if not first:
                    mine = mine + gu[span, lanes]
                gu[span, lanes] = mine.astype(BF16).astype(F32) if last_of else mine

    far_t, right_t, left_t = turns[0], turns[1], turns[2]
    whole, inner, outer = range(8), (0, 1, -1), (2, -2)
    rest = (3, -3, 4)
    gather(("x_piece", -3), ("pair_done", 0), ("pair_done", 1), ("pair_done", -1))
    own = (chunk(y),)
    mark("project_own")
    project(own, inner, True, False)
    gather(("x_piece", 3), ("x_far", -2), ("x_far", 2), ("z_group", 3, 0, 1, 2, 3))
    gather(("x_piece", 4))
    mark("all_first")
    v = nall.at[chunk_half(left_t, 0)]
    wire.arrive(v, all_sem.at[0, 0], left)
    wire.send(v, v, right, all_sem.at[2, 0])
    v = nall.at[chunk_half(right_t, 1)]
    wire.arrive(v, all_sem.at[1, 1], right)
    wire.send(v, v, left, all_sem.at[2, 1])
    gather(("x_far", -3), ("x_far", 3), ("pair_done", 2), ("pair_done", -2))
    mark("project_own2")
    project(own, outer, False, False)
    gather(("x_far", 4),)
    mark("near_wait")
    wire.arrive(nall.at[chunk_half(left_t, 1)], all_sem.at[0, 1], left)
    wire.arrive(nall.at[chunk_half(right_t, 0)], all_sem.at[1, 0], right)
    near = (chunk(left_t), chunk(right_t))
    mark("project_near")
    project(near, inner + outer, True, False)
    gather(("z_group", 4, 0, 1, 2, 3), ("pair_done", 3), ("pair_done", -3), ("pair_done", 4))
    mark("project_rest")
    project(own + near, rest, False, True)
    mark("far_wait")
    wire.arrive(nall.at[chunk_half(far_t, 0)], all_sem.at[2, 0], left)
    wire.arrive(nall.at[chunk_half(far_t, 1)], all_sem.at[2, 1], right)
    mark("halo")

    @pl.when(has_last)
    def _():
        wire.arrive(nall.at[pl.ds(0, 16)], all_sem.at[3, 0], rank_dev(before, 3))

    @pl.when(jnp.logical_not(has_last))
    def _():
        nall[0:16] = jnp.zeros((16, D), BF16)
    mark("project_far")
    project((chunk(far_t), pl.ds(0, 16)), whole, True, True)

    def conv_gu(t, lanes, taps, tap_lanes):
        window = gu[pl.ds(pl.multiple_of(t * BLOCK + 8, 8), BLOCK + 8), lanes]
        weights = taps[:, tap_lanes].astype(F32)
        total = weights[0:1] * window[6 : 6 + BLOCK]
        for k in range(1, 3):
            total = total + weights[k : k + 1] * window[6 + k : 6 + k + BLOCK]
        return total

    def ffn_part(k):
        t = turns[k]
        pieces = []
        for j in range(11):
            lanes = slice(j * 128, (j + 1) * 128)
            shifted_lanes = slice(FF + j * 128, FF + (j + 1) * 128)
            gate = conv_gu(t, lanes, gate_taps, lanes)
            pieces.append((silu(gate) * conv_gu(t, shifted_lanes, up_taps, lanes)).astype(BF16))
        hidden = jnp.concatenate(pieces, axis=1)

        def tile(j):
            w = wv[2 * j : 2 * j + 2, :, :, :, 2 * FF :].reshape(512, FF)
            ffn_out[k, :, j * 512 : (j + 1) * 512] = lax.dot_general(
                hidden, w, NT, preferred_element_type=F32
            ).astype(BF16)

        return tile

    channel = reduce_rows(ffn_part, ffn_out, ffn_far, ffn_in, ffn_sem, lambda stage: None, "ffn")
    mark("norm_two")
    out[...] = layer_norm(
        ALPHA * nall[chunk(y), :].astype(F32) + channel, scale_two[...]
    ).astype(BF16)
    mark("finish")
    wire.finish()
    mark.end()


def shards(*arrays):
    arrays = [a.reshape(1, -1) if a.ndim == 1 else a for a in arrays]
    for k in (5, 8, 18):
        arrays[k] = arrays[k].T
    dma = pltpu.SemaphoreType.DMA
    loaded = arrays[:16] + arrays[19:]
    scratch = [pltpu.VMEM(a.shape, a.dtype) for a in loaded] + [
        pltpu.VMEM((8, 4, 2, 32, COLS), BF16),
        dma((22,)),
        pltpu.VMEM((16, INNER), BF16),
        pltpu.VMEM((16, STATE), BF16),
        pltpu.VMEM((16, STATE), BF16),
        pltpu.VMEM((ROWS, INNER), BF16),
        pltpu.VMEM((ROWS, STATE), BF16),
        pltpu.VMEM((ROWS, STATE), BF16),
        pltpu.VMEM((ROWS, 128), F32),
        pltpu.VMEM((BLOCKS, 2 * HEADS, BLOCK), F32),
        pltpu.VMEM((ROWS, INNER), F32),
        pltpu.VMEM((ROWS, INNER), F32),
        pltpu.VMEM((BLOCKS, STATE, INNER), F32),
        pltpu.VMEM((BLOCKS, 8, INNER), F32),
        pltpu.VMEM((STATE, INNER), BF16),
        pltpu.VMEM((8, 16, INNER), BF16),
        pltpu.VMEM((8, 4, 128), F32),
        pltpu.VMEM((8, 16, INNER), F32),
        pltpu.VMEM((8, 8, INNER), F32),
        pltpu.VMEM((4, 128), F32),
        pltpu.VMEM((8, 16, INNER), BF16),
        pltpu.VMEM((8, 4, 128), F32),
        pltpu.VMEM((16, INNER), BF16),
        pltpu.VMEM((4, 128), F32),
        pltpu.VMEM((16, INNER), F32),
        pltpu.VMEM((8, 16, INNER), BF16),
        pltpu.VMEM((STATE, INNER), BF16),
        pltpu.VMEM((4, BLOCK, D), BF16),
        pltpu.VMEM((2, 64, D), BF16),
        pltpu.VMEM((2, BLOCK, D), BF16),
        pltpu.VMEM((ROWS + 16, D), BF16),
        pltpu.VMEM((ROWS + 16, 2 * FF), F32),
        pltpu.VMEM((4, BLOCK, D), BF16),
        pltpu.VMEM((2, 64, D), BF16),
        pltpu.VMEM((2, BLOCK, D), BF16),
        dma((260,)),
        dma((86,)),
        dma((8,)),
        dma((3,)),
        dma((2, 8)),
        dma((2, 8)),
        dma((8,)),
        dma((18,)),
        dma((4, 2)),
        dma((18,)),
    ]
    return pl.pallas_call(
        layer_kernel,
        out_shape=jax.ShapeDtypeStruct((BLOCK, D), BF16),
        in_specs=[pl.BlockSpec(memory_space=pltpu.HBM)] * len(arrays),
        out_specs=pl.BlockSpec(memory_space=pltpu.VMEM),
        scratch_shapes=scratch,
        compiler_params=pltpu.CompilerParams(
            collective_id=0, has_side_effects=True, vmem_limit_bytes=67043328
        ),
    )(*arrays)


def solution(mesh):
    split = Mesh(mesh.devices.reshape(8, 4, 2, mesh.shape["tp"]), ("sp_0", "sp_1", "sp_2", "tp"))
    in_specs = (
        P(SP_TP, None),
        P(SP, "tp"),
        P(SP, "tp"),
        P(SP, "tp"),
        P(SP, "tp"),
        P(SP, "tp"),
        P("tp"),
        P("tp"),
        P(SP, "tp"),
        P("tp"),
        P(None, "tp"),
        P(None, "tp"),
        P(None, "tp"),
        P("tp"),
        P("tp", None),
        P(),
        P(SP, "tp"),
        P(SP, "tp"),
        P("tp", SP),
        P(None, "tp"),
        P(None, "tp"),
        P(),
    )
    out_specs = P(SP_TP, None)
    return jax.shard_map(
        shards, mesh=split, in_specs=in_specs, out_specs=out_specs, check_vma=False
    )
```

```python
import jax
import jax.numpy as jnp
from jax import lax
from jax.experimental import pallas as pl
from jax.experimental.pallas import tpu as pltpu
from jax.sharding import Mesh
from jax.sharding import PartitionSpec as P

HEADS = 8
HEAD_DIM = 64
STATE = 128
BLOCK = 128
BLOCKS = 4
ROWS = BLOCK * BLOCKS
INNER = 512
D = 2048
FF = 1408
COLS = 3 * FF
NA = 1792
EPSILON = 1e-05
ALPHA = 2.0**0.25
SP = ("sp_0", "sp_1", "sp_2")
SP_TP = ("sp_0", "sp_1", "sp_2", "tp")
MESH = pl.DeviceIdType.MESH
F32 = jnp.float32
BF16 = jnp.bfloat16
NT = (((1,), (1,)), ((), ()))


def wrap(value, count):
    return lax.rem(value + 2 * count, count)


class Marks:
    def __init__(self):
        self.scope = None

    def __call__(self, name):
        self.end()
        self.scope = jax.named_scope(name)
        self.scope.__enter__()

    def end(self):
        if self.scope is not None:
            self.scope.__exit__(None, None, None)
            self.scope = None


class Wire:
    def __init__(self, send_sem):
        self.send_sem = send_sem
        self.count = 0
        self.waits = []

    def send(self, src, dst, dev, recv_sem, when=None):
        copy = pltpu.make_async_remote_copy(
            src_ref=src,
            dst_ref=dst,
            send_sem=self.send_sem.at[self.count],
            recv_sem=recv_sem,
            device_id=dev,
            device_id_type=MESH,
        )
        self.count += 1
        if when is None:
            copy.start()
        else:
            pl.when(when)(copy.start)
        self.waits.append((copy, when))

    def arrive(self, dst, recv_sem, dev):
        pltpu.make_async_remote_copy(
            src_ref=dst,
            dst_ref=dst,
            send_sem=self.send_sem.at[0],
            recv_sem=recv_sem,
            device_id=dev,
            device_id_type=MESH,
        ).wait_recv()

    def finish(self):
        for copy, when in self.waits:
            if when is None:
                copy.wait_send()
            else:
                pl.when(when)(copy.wait_send)


def weight_gather(wire, wv, rsem, psem, ids, mark):
    z, x, c, _ = ids
    cols_a, cols_b = pl.ds(0, NA), pl.ds(NA, COLS - NA)
    half, whole = (pl.ds(0, 16), pl.ds(16, 16)), pl.ds(0, 32)
    zp, zm = {"sp_0": wrap(z + 1, 8)}, {"sp_0": wrap(z - 1, 8)}
    xp, xm = {"sp_1": wrap(x + 1, 4)}, {"sp_1": wrap(x - 1, 4)}
    other = {"sp_2": 1 - c}
    xl, xr, xf = wrap(x - 1, 4), wrap(x + 1, 4), wrap(x + 2, 4)

    def pair(off):
        return psem.at[off % 8]

    def piece(zz, xx, cols, rows=whole):
        return wv.at[zz, xx, c, rows, cols]

    def group(zz, rows=whole):
        return wv.at[zz, :, c, rows, cols_a]

    def send(view, dev, sem):
        wire.send(view, view, dev, sem)

    def arrive(view, sem):
        wire.arrive(view, sem, other)

    def a1(d, h):
        return rsem.at[d * 2 + h]

    def a1f(d):
        return rsem.at[4 + d]

    def b1(d, s):
        return rsem.at[14 + d * 4 + s - 1]

    def b2(d, s):
        return rsem.at[22 + d * 8 + s]

    def b2f(d, s):
        return rsem.at[38 + d * 8 + s]

    def a2(d, s, k):
        return rsem.at[54 + d * 16 + (s - 1) * 4 + k]

    columns = (x, xl, xr, xf)

    def x_send(off):
        v = piece(wrap(z + off, 8), x, cols_b)
        send(v, xp, b2(0, off % 8))
        send(v, xm, b2(1, off % 8))

    def start():
        send(piece(z, x, cols_a, half[0]), xp, a1(0, 0))
        send(piece(z, x, cols_a, half[1]), xm, a1(1, 1))
        send(piece(z, x, cols_a, half[1]), xp, a1(0, 1))
        send(piece(z, x, cols_a, half[0]), xm, a1(1, 0))
        send(piece(z, x, cols_b), zp, b1(0, 1))
        send(piece(z, x, cols_b), zm, b1(1, 1))
        send(piece(z, x, cols_a), zp, a2(0, 1, 0))
        send(piece(z, x, cols_a), zm, a2(1, 1, 0))
        send(piece(z, x, cols_b), other, pair(0))

    def row_far():
        v = piece(z, xl, cols_a, half[0])
        arrive(v, a1(0, 0))
        send(v, xp, a1f(0))
        v = piece(z, xr, cols_a, half[1])
        arrive(v, a1(1, 1))
        send(v, xm, a1f(1))

    def row_done():
        arrive(piece(z, xl, cols_a, half[1]), a1(0, 1))
        arrive(piece(z, xr, cols_a, half[0]), a1(1, 0))
        arrive(piece(z, xf, cols_a, half[0]), a1f(0))
        arrive(piece(z, xf, cols_a, half[1]), a1f(1))
        for k in range(1, 4):
            send(piece(z, columns[k], cols_a), zp, a2(0, 1, k))
            send(piece(z, columns[k], cols_a), zm, a2(1, 1, k))
        send(group(z), other, pair(0))

    def z_piece(s):
        zl, zr = wrap(z - s, 8), wrap(z + s, 8)
        if s < 4:
            v = piece(zl, x, cols_b)
            arrive(v, b1(0, s))
            send(v if s < 3 else piece(zl, x, cols_b, half[0]), zp, b1(0, s + 1))
            send(v, other, pair(-s))
            v = piece(zr, x, cols_b)
            arrive(v, b1(1, s))
            send(v if s < 3 else piece(zr, x, cols_b, half[1]), zm, b1(1, s + 1))
            send(v, other, pair(s))
        else:
            arrive(piece(zl, x, cols_b, half[0]), b1(0, 4))
            arrive(piece(zl, x, cols_b, half[1]), b1(1, 4))
            send(piece(zl, x, cols_b), other, pair(4))

    def z_group(s, *which):
        zl, zr = wrap(z - s, 8), wrap(z + s, 8)
        for k in which:
            if s < 4:
                v = piece(zl, columns[k], cols_a)
                arrive(v, a2(0, s, k))
                send(v if s < 3 else piece(zl, columns[k], cols_a, half[0]), zp, a2(0, s + 1, k))
                v = piece(zr, columns[k], cols_a)
                arrive(v, a2(1, s, k))
                send(v if s < 3 else piece(zr, columns[k], cols_a, half[1]), zm, a2(1, s + 1, k))
            else:
                arrive(piece(zl, columns[k], cols_a, half[0]), a2(0, 4, k))
                arrive(piece(zl, columns[k], cols_a, half[1]), a2(1, 4, k))
        if 3 in which:
            send(group(zl), other, pair(-s))
            if s < 4:
                send(group(zr), other, pair(s))

    def x_piece(off):
        zz = wrap(z + off, 8)
        v = piece(zz, xl, cols_b)
        arrive(v, b2(0, off % 8))
        send(piece(zz, xl, cols_b, half[0]), xp, b2f(0, off % 8))
        send(v, other, pair(off))
        v = piece(zz, xr, cols_b)
        arrive(v, b2(1, off % 8))
        send(piece(zz, xr, cols_b, half[1]), xm, b2f(1, off % 8))
        send(v, other, pair(off))

    def x_far(off):
        zz = wrap(z + off, 8)
        arrive(piece(zz, xf, cols_b, half[0]), b2f(0, off % 8))
        arrive(piece(zz, xf, cols_b, half[1]), b2f(1, off % 8))
        send(piece(zz, xf, cols_b), other, pair(off))

    def pair_done(off):
        arrive(wv.at[wrap(z + off, 8), :, 1 - c], pair(off))

    steps = {
        "start": start,
        "row_far": row_far,
        "row_done": row_done,
        "z_piece": z_piece,
        "z_group": z_group,
        "x_send": x_send,
        "x_piece": x_piece,
        "x_far": x_far,
        "pair_done": pair_done,
    }

    def run(*plan):
        for name, *at in plan:
            mark("g_" + name + "".join(str(k) for k in at))
            steps[name](*at)

    return run


def thirds(v):
    high = v.astype(BF16)
    rest = v - high.astype(F32)
    mid = rest.astype(BF16)
    return high, mid, (rest - mid.astype(F32)).astype(BF16)


def dot(a, b):
    return jnp.dot(a, b, preferred_element_type=F32)


def spread(v, onehot):
    return sum(dot(part, onehot) for part in thirds(v))


def silu(v):
    return v * (1.0 / (1.0 + jnp.exp(-v)))


def layer_norm(values, scales):
    centred = values - jnp.mean(values, axis=-1, keepdims=True)
    spread_of = jnp.mean(centred * centred, axis=-1, keepdims=True)
    return centred * lax.rsqrt(spread_of + EPSILON) * scales


LOADED = (
    "resid",
    "valve",
    "x_in",
    "b_in",
    "c_in",
    "deltas",
    "offset",
    "speed",
    "fading",
    "bypass",
    "x_taps",
    "b_taps",
    "c_taps",
    "cluster",
    "w_mix",
    "scale_one",
    "gate_taps",
    "up_taps",
    "scale_two",
)


EARLY = LOADED[2:13]


def layer_kernel(*refs):
    sources, out, refs = refs[:22], refs[22], refs[23:]
    loads, refs = refs[:19], refs[19:]
    (
        resid,
        valve,
        x_in,
        b_in,
        c_in,
        deltas,
        offset,
        speed,
        fading,
        bypass,
        x_taps,
        b_taps,
        c_taps,
        cluster,
        w_mix,
        scale_one,
        gate_taps,
        up_taps,
        scale_two,
    ) = loads
    (
        wv,
        load_sem,
        x_rim,
        b_rim,
        c_rim,
        xs,
        bs,
        cs,
        cums,
        turned,
        ec,
        yw,
        states,
        decays,
        ends,
        row_ends,
        row_decay,
        row_pre,
        row_dpre,
        own_decay,
        z_state,
        z_decay,
        z_out,
        z_dout,
        z_acc,
        to_row,
        incoming,
        gated,
        far_rows,
        near_rows,
        far_out,
        far_got,
        mixed,
        w_near,
        nall,
        tail_out,
        tail_in,
        gu,
        ffn_out,
        ffn_far_in,
        ffn_in,
        ffn_mixed,
        send_sem,
        gather_sem,
        pair_sem,
        rim_sem,
        row_sem,
        z_sem,
        back_sem,
        mix_sem,
        near_sem,
        all_sem,
        ffn_sem,
    ) = refs
    ids = tuple(lax.axis_index(name) for name in SP_TP)
    z, x, c, y = ids
    rank = z * 8 + x * 2 + c
    place = x * 2 + c
    wire = Wire(send_sem)

    def rank_dev(r, tp=None):
        dev = {"sp_0": lax.div(r, 8), "sp_1": lax.div(lax.rem(r, 8), 2), "sp_2": lax.rem(r, 2)}
        if tp is not None:
            dev["tp"] = tp
        return dev

    def row_dev(p):
        return {"sp_1": lax.div(p, 2), "sp_2": lax.rem(p, 2)}

    after, before = wrap(rank + 1, 64), wrap(rank - 1, 64)
    right, left = {"tp": wrap(y + 1, 4)}, {"tp": wrap(y - 1, 4)}

    mark = Marks()
    mark("barrier")
    sem = pltpu.get_barrier_semaphore()
    greeted = [{"sp_0": wrap(z + k, 8)} for k in range(1, 8)]
    greeted += [row_dev(wrap(place + k, 8)) for k in range(1, 8)]
    greeted += [right, left]
    greeted += [rank_dev(before, k) for k in range(4)]
    for dev in greeted:
        pl.semaphore_signal(sem, inc=1, device_id=dev, device_id_type=MESH)

    sources, shards_here = sources[:16] + sources[19:], sources[16:19]
    copies = [
        pltpu.make_async_copy(src, wv.at[z, x, c, :, pl.ds(k * FF, FF)], load_sem.at[19 + k])
        for k, src in enumerate(shards_here)
    ]
    order = sorted(range(19), key=lambda k: LOADED[k] not in EARLY)
    copies += [pltpu.make_async_copy(sources[k], loads[k], load_sem.at[k]) for k in order]
    for copy in copies:
        copy.start()
    for copy in copies[: 3 + len(EARLY)]:
        copy.wait()
    pl.semaphore_wait(sem, len(greeted))

    has_next, has_last = rank < 63, rank > 0
    last = pl.ds(ROWS - 16, 16)
    for k, (src, dst) in enumerate(((x_in, x_rim), (b_in, b_rim), (c_in, c_rim))):
        wire.send(src.at[last], dst, rank_dev(after), rim_sem.at[k], when=has_next)
    gather = weight_gather(wire, wv, gather_sem, pair_sem, ids, mark)
    gather(("start",))
    w_source = sources[LOADED.index("w_mix")]

    def w_rows(core, k):
        return pl.ds(pl.multiple_of(core * 256 + k * 64, 64), 64)

    for k in range(4):
        for d, dev in enumerate((right, left)):
            rows_k = w_rows(c, k)
            wire.send(w_source.at[rows_k], w_near.at[d, rows_k], dev, near_sem.at[d, k])

    def pass_on(k):
        mark("w_pass" + str(k))
        for d, dev in enumerate((left, right)):
            v = w_near.at[d, w_rows(c, k)]
            wire.arrive(v, near_sem.at[d, k], dev)
            wire.send(v, v, {"sp_2": 1 - c}, near_sem.at[2 + d, k])

    def w_whole():
        mark("w_whole")
        for k in range(4):
            for d in range(2):
                wire.arrive(w_near.at[d, w_rows(1 - c, k)], near_sem.at[2 + d, k], {"sp_2": 1 - c})

    rows_at = lax.broadcasted_iota(jnp.int32, (BLOCK, BLOCK), 0)
    cols_at = lax.broadcasted_iota(jnp.int32, (BLOCK, BLOCK), 1)
    causal = rows_at >= cols_at
    triu = (rows_at <= cols_at).astype(BF16)
    onehot = (
        lax.broadcasted_iota(jnp.int32, (HEADS, INNER), 0)
        == lax.div(lax.broadcasted_iota(jnp.int32, (HEADS, INNER), 1), HEAD_DIM)
    ).astype(BF16)
    eye = lax.broadcasted_iota(jnp.int32, (HEADS, HEADS), 0) == lax.broadcasted_iota(
        jnp.int32, (HEADS, HEADS), 1
    )

    def turned_up(v):
        return jnp.sum(
            jnp.where(eye, jnp.broadcast_to(v[...], (HEADS, HEADS)), 0.0), axis=1, keepdims=True
        )

    offset_col, speed_col = turned_up(offset), turned_up(speed)
    skip = spread(jnp.broadcast_to(bypass[...], (8, HEADS)), onehot)[0:1]
    low_lanes = lax.broadcasted_iota(jnp.int32, (BLOCK, 2 * HEAD_DIM), 1) < HEAD_DIM

    def conv_block(src, rim, taps, b):
        if b == 0:
            window = jnp.concatenate([rim[...], src[0:BLOCK]], axis=0).astype(F32)
        else:
            window = src[b * BLOCK - 16 : (b + 1) * BLOCK].astype(F32)
        weights = taps[...].astype(F32)
        total = weights[0:1] * window[13 : 13 + BLOCK]
        for k in range(1, 4):
            total = total + weights[k : k + 1] * window[13 + k : 13 + k + BLOCK]
        return silu(total)

    def local_block(b):
        span = slice(b * BLOCK, (b + 1) * BLOCK)
        x_act = conv_block(x_in, x_rim, x_taps, b).astype(BF16)
        b_act = conv_block(b_in, b_rim, b_taps, b).astype(BF16)
        xs[span] = x_act
        bs[span] = b_act
        raw = deltas[:, span] + offset_col
        step_rows = jnp.maximum(raw, 0.0) + jnp.log1p(jnp.exp(-jnp.abs(raw)))
        cum_rows = spread(fading[:, span] - speed_col * step_rows, triu)
        both = jnp.concatenate([cum_rows, step_rows], axis=0)
        turned[b] = both
        both = jnp.concatenate([both, jnp.zeros((112, BLOCK), F32)], axis=0).T
        cums[span] = both
        cum, step = both[:, 0:HEADS], both[:, HEADS : 2 * HEADS]
        grown = spread(jnp.broadcast_to(jnp.exp(cum[BLOCK - 1 : BLOCK]), (8, HEADS)), onehot)
        to_end = spread(step * jnp.exp(cum[BLOCK - 1 : BLOCK] - cum), onehot)
        weighted = (x_act.astype(F32) * to_end).astype(BF16)
        states[b] = dot(b_act.astype(F32).T.astype(BF16), weighted)
        decays[b] = grown

    def readout_block(b):
        span = slice(b * BLOCK, (b + 1) * BLOCK)
        cs[span] = conv_block(c_in, c_rim, c_taps, b).astype(BF16)
        ec[span] = spread(jnp.exp(cums[span, 0:HEADS]), onehot)

    def within_block(b):
        span = slice(b * BLOCK, (b + 1) * BLOCK)
        affinity = lax.dot_general(cs[span], bs[span], NT, preferred_element_type=F32)
        for pair in range(HEADS // 2):
            lanes = slice(pair * 128, (pair + 1) * 128)
            mixing = []
            for h in (2 * pair, 2 * pair + 1):
                between = cums[span, h : h + 1] - turned[b, h : h + 1]
                lag = jnp.exp(jnp.where(causal, between, -1e30))
                mixing.append((affinity * lag * turned[b, HEADS + h : HEADS + h + 1]).astype(BF16))
            x_pair = xs[span, lanes]
            zero = jnp.zeros_like(x_pair)
            sides = jnp.concatenate(
                [jnp.where(low_lanes, x_pair, zero), jnp.where(low_lanes, zero, x_pair)], axis=0
            )
            yw[span, lanes] = dot(jnp.concatenate(mixing, axis=1), sides) + skip[
                :, lanes
            ] * x_pair.astype(F32)

    def packed(v):
        return jnp.concatenate([v[:, k * 128 : (k + 1) * 128] for k in range(4)], axis=0)

    def unpacked(tile):
        return jnp.concatenate([tile[k : k + 1] for k in range(4)], axis=1)

    mark("local3")
    local_block(3)
    mark("local2")
    local_block(2)
    local_block(1)
    mark("rim_wait")

    @pl.when(has_last)
    def _():
        for k, dst in enumerate((x_rim, b_rim, c_rim)):
            wire.arrive(dst, rim_sem.at[k], rank_dev(before))

    @pl.when(jnp.logical_not(has_last))
    def _():
        for dst in (x_rim, b_rim, c_rim):
            dst[...] = jnp.zeros_like(dst)

    mark("local0")
    local_block(0)
    mark("ends")

    total = jnp.zeros((STATE, INNER), F32)
    growth = jnp.ones((1, INNER), F32)
    for b in range(BLOCKS):
        fresh, decay = states[b], decays[b, 0:1]
        states[b] = total
        decays[b] = jnp.broadcast_to(growth, (8, INNER))
        total = total * decay + fresh
        growth = growth * decay
    ends[...] = total.astype(BF16)
    own_decay[...] = packed(growth)

    def sixteen(p):
        return pl.ds(pl.multiple_of(p * 16, 16), 16)

    for k in range(1, 8):
        to = wrap(place + k, 8)
        wire.send(ends.at[sixteen(to)], row_ends.at[place], row_dev(to), row_sem.at[0, k])
        wire.send(own_decay, row_decay.at[place], row_dev(to), row_sem.at[1, k])
    row_ends[place] = ends[sixteen(place), :]
    row_decay[place] = own_decay[...]
    gather(("row_far",), ("x_send", 0), ("z_piece", 1))
    mark("within01")
    readout_block(0)
    readout_block(1)
    within_block(0)
    within_block(1)
    mark("row_wait")
    for k in range(1, 8):
        src = wrap(place - k, 8)
        wire.arrive(row_ends.at[src], row_sem.at[0, k], row_dev(src))
        wire.arrive(row_decay.at[src], row_sem.at[1, k], row_dev(src))
    pass_on(0)
    mark("row_fold")
    total = jnp.zeros((16, INNER), F32)
    growth = jnp.ones((1, INNER), F32)
    for q in range(8):
        decay = unpacked(row_decay[q])
        row_pre[q] = total
        row_dpre[q] = jnp.broadcast_to(growth, (8, INNER))
        total = total * decay + row_ends[q].astype(F32)
        growth = growth * decay
    z_out[...] = total.astype(BF16)
    z_dout[...] = packed(growth)
    for k in range(1, 8):
        to = {"sp_0": wrap(z + k, 8)}
        wire.send(z_out, z_state.at[k], to, z_sem.at[0, k], when=z + k < 8)
        wire.send(z_dout, z_decay.at[k], to, z_sem.at[1, k], when=z + k < 8)
    gather(("x_send", -1), ("row_done",))
    mark("within23")
    readout_block(2)
    readout_block(3)
    within_block(2)
    within_block(3)
    mark("z_wait")
    z_acc[...] = jnp.zeros_like(z_acc)
    for k in range(7, 0, -1):

        @pl.when(z >= k)
        def _():
            src = {"sp_0": wrap(z - k, 8)}
            wire.arrive(z_state.at[k], z_sem.at[0, k], src)
            wire.arrive(z_decay.at[k], z_sem.at[1, k], src)
            z_acc[...] = z_acc[...] * unpacked(z_decay[k]) + z_state[k].astype(F32)

    mark("z_fold")
    begun = z_acc[...]
    for q in range(8):
        to_row[q] = (begun * row_dpre[q, 0:1] + row_pre[q]).astype(BF16)
    for k in range(1, 8):
        to = wrap(place + k, 8)
        wire.send(to_row.at[to], incoming.at[sixteen(place)], row_dev(to), back_sem.at[k])
    incoming[sixteen(place), :] = to_row[place]
    gather(("x_send", 1), ("x_piece", 0), ("z_piece", 2))
    mark("back_wait")
    for k in range(1, 8):
        src = wrap(place - k, 8)
        wire.arrive(incoming.at[sixteen(src)], back_sem.at[k], row_dev(src))

    for copy in copies[3 + len(EARLY) :]:
        copy.wait()
    turns = [wrap(y + 2, 4), wrap(y + 1, 4), wrap(y - 1, 4), y]

    def gated_block(t):
        span = pl.ds(pl.multiple_of(t * BLOCK, BLOCK), BLOCK)
        begin = states[t] + incoming[...].astype(F32) * decays[t, 0:1]
        gated = yw[span, :] + ec[span, :] * dot(cs[span, :], begin.astype(BF16))
        gated = gated * silu(valve[span, :].astype(F32))
        gated = gated * lax.rsqrt(jnp.mean(gated * gated, axis=-1, keepdims=True) + EPSILON)
        return (gated * cluster[...]).astype(BF16)

    mark("mix_blocks")
    gated[0] = gated_block(turns[0])
    wire.send(gated.at[0, pl.ds(0, 64)], far_rows.at[0], right, mix_sem.at[0])
    wire.send(gated.at[0, pl.ds(64, 64)], far_rows.at[1], left, mix_sem.at[1])
    gated[1] = gated_block(turns[1])
    wire.send(gated.at[1], near_rows.at[0], right, mix_sem.at[2])
    gated[2] = gated_block(turns[2])
    wire.send(gated.at[2], near_rows.at[1], left, mix_sem.at[3])
    pass_on(1)
    pass_on(2)
    mark("mix_own")
    mixed[...] = dot(gated_block(y), w_mix[...])
    gather(("x_send", -2), ("x_send", 2), ("z_group", 1, 0, 1), ("x_piece", -1), ("z_group", 1, 2, 3))
    pass_on(3)
    w_whole()
    mark("mix_far_wait")
    wire.arrive(far_rows.at[0], mix_sem.at[0], left)
    wire.arrive(far_rows.at[1], mix_sem.at[1], right)
    mark("mix_far")
    for j in range(4):
        lanes = pl.ds(j * 512, 512)
        for d, dev in enumerate((right, left)):
            far_out[d, :, j * 512 : (j + 1) * 512] = dot(
                far_rows[d], w_near[d, :, j * 512 : (j + 1) * 512]
            ).astype(BF16)
            wire.send(far_out.at[d, :, lanes], far_got.at[d, :, lanes], dev, mix_sem.at[4 + 4 * d + j])
    gather(("z_piece", 3), ("x_piece", 1), ("x_send", -3), ("x_send", 3))
    mark("mix_near_wait")
    wire.arrive(near_rows.at[0], mix_sem.at[2], left)
    wire.arrive(near_rows.at[1], mix_sem.at[3], right)
    mark("mix_near")
    for d in range(2):
        mixed[...] += dot(near_rows[d], w_near[d])
    gather(("x_piece", -2), ("x_far", 0))
    mark("mix_wait")
    for j in range(4):
        lanes = pl.ds(j * 512, 512)
        for d, dev in enumerate((left, right)):
            wire.arrive(far_got.at[d, :, lanes], mix_sem.at[4 + 4 * d + j], dev)
    mark("norm_one")
    far_sum = jnp.concatenate([far_got[0], far_got[1]], axis=0).astype(F32)
    mixer = mixed[...] + far_sum
    normed = layer_norm(ALPHA * resid[...].astype(F32) + mixer, scale_one[...]).astype(BF16)

    def chunk(t):
        return pl.ds(pl.multiple_of(16 + t * BLOCK, 16), BLOCK)

    def chunk_half(t, h):
        return pl.ds(pl.multiple_of(16 + t * BLOCK + h * 64, 16), 64)

    nall[chunk(y), :] = normed
    tail = normed[BLOCK - 16 :].astype(F32)[14:16]
    tail_out[...] = jnp.concatenate(
        [tail[:, k * 128 : (k + 1) * 128] for k in range(16)], axis=0
    ).astype(BF16)
    for k in range(4):
        wire.send(
            tail_out,
            tail_in,
            rank_dev(after, k),
            all_sem.at[3, 0],
            when=jnp.logical_and(has_next, y == 3),
        )
    mark("all_send")
    for h in range(2):
        for dev, half_of in ((right, h), (left, 1 - h)):
            v = nall.at[chunk_half(y, half_of)]
            wire.send(v, v, dev, all_sem.at[0 if dev is right else 1, half_of])
    def project(spans, offs, first, last_of):
        zs = [wrap(z + off, 8) for off in offs]
        deep = [pl.ds(pl.multiple_of(zz * 256, 256), 256) for zz in zs]
        rows = jnp.concatenate(
            [jnp.concatenate([nall[span, k] for k in deep], axis=1) for span in spans], axis=0
        )

        for j in range(11):
            lanes = slice(j * 256, (j + 1) * 256)
            weights = [wv[zz, :, :, :, lanes].reshape(256, 256) for zz in zs]
            got = dot(rows, jnp.concatenate(weights, axis=0))
            at = 0
            for span in spans:
                mine = got[at : at + span.size]
                at += span.size
                if not first:
                    mine = mine + gu[span, lanes]
                gu[span, lanes] = mine.astype(BF16).astype(F32) if last_of else mine

    far_t, right_t, left_t = turns[0], turns[1], turns[2]
    def hidden_rows(pieces):
        columns = []
        for j in range(11):
            lanes = slice(j * 128, (j + 1) * 128)
            up_lanes = slice(FF + j * 128, FF + (j + 1) * 128)
            rows = []
            for t, first, count in pieces:
                at = pl.ds(pl.multiple_of(t * BLOCK + first + 8, 8), count + 8)
                sums = []
                for source, taps in ((lanes, gate_taps), (up_lanes, up_taps)):
                    window = gu[at, source]
                    weights = taps[:, lanes].astype(F32)
                    total = weights[0:1] * window[6 : 6 + count]
                    for k in range(1, 3):
                        total = total + weights[k : k + 1] * window[6 + k : 6 + k + count]
                    sums.append(total)
                rows.append((silu(sums[0]) * sums[1]).astype(BF16))
            columns.append(rows[0] if len(rows) == 1 else jnp.concatenate(rows, axis=0))
        return jnp.concatenate(columns, axis=1)

    def down(hidden, j):
        w = wv[2 * j : 2 * j + 2, :, :, :, 2 * FF :].reshape(512, FF)
        return lax.dot_general(hidden, w, NT, preferred_element_type=F32)

    upper, lower = pl.ds(0, 64), pl.ds(64, 64)
    tiles = [(j, pl.ds(j * 512, 512), slice(j * 512, (j + 1) * 512)) for j in range(4)]

    def ffn_near():
        mark("ffn_near")
        hidden = hidden_rows(((right_t, 0, 64), (left_t, 64, 64)))
        for j, lanes, at in tiles:
            ffn_out[0, :, at] = down(hidden, j).astype(BF16)
            wire.send(ffn_out.at[0, upper, lanes], ffn_in.at[0, upper, lanes], right, ffn_sem.at[j])
            wire.send(
                ffn_out.at[0, lower, lanes], ffn_in.at[1, lower, lanes], left, ffn_sem.at[4 + j]
            )

    def ffn_far():
        mark("ffn_far")
        hidden = hidden_rows(((far_t, 0, 128),))
        for j, lanes, at in tiles:
            ffn_out[1, :, at] = down(hidden, j).astype(BF16)
            wire.send(ffn_out.at[1, lower, lanes], ffn_far_in.at[0, :, lanes], right, ffn_sem.at[8 + j])
            wire.send(ffn_out.at[1, upper, lanes], ffn_far_in.at[1, :, lanes], left, ffn_sem.at[12 + j])

    def ffn_last():
        mark("ffn_mixed")
        hidden = hidden_rows(((right_t, 64, 64), (left_t, 0, 64)))
        for j, lanes, at in tiles:
            ffn_mixed[:, at] = down(hidden, j)
        mark("ffn_far_wait")
        for j, lanes, at in tiles:
            wire.arrive(ffn_far_in.at[0, :, lanes], ffn_sem.at[8 + j], left)
            wire.arrive(ffn_far_in.at[1, :, lanes], ffn_sem.at[12 + j], right)
            both = jnp.concatenate([ffn_far_in[0, :, at], ffn_far_in[1, :, at]], axis=0)
            ffn_out[2, :, at] = (ffn_mixed[:, at] + both.astype(F32)).astype(BF16)
            wire.send(
                ffn_out.at[2, upper, lanes], ffn_in.at[0, lower, lanes], right, ffn_sem.at[16 + j]
            )
            wire.send(
                ffn_out.at[2, lower, lanes], ffn_in.at[1, upper, lanes], left, ffn_sem.at[20 + j]
            )
        mark("ffn_own")
        hidden = hidden_rows(((y, 0, 128),))
        for j, lanes, at in tiles:
            ffn_mixed[:, at] = down(hidden, j)
        mark("ffn_wait")
        for j, lanes, at in tiles:
            wire.arrive(ffn_in.at[0, upper, lanes], ffn_sem.at[j], left)
            wire.arrive(ffn_in.at[1, lower, lanes], ffn_sem.at[4 + j], right)
            wire.arrive(ffn_in.at[0, lower, lanes], ffn_sem.at[16 + j], left)
            wire.arrive(ffn_in.at[1, upper, lanes], ffn_sem.at[20 + j], right)
        mark("norm_two")
        return ffn_mixed[...] + ffn_in[0].astype(F32) + ffn_in[1].astype(F32)

    inner, outer = (0, 1, -1), (2, -2)
    rest = (3, -3, 4)
    gather(("x_piece", 2), ("z_group", 2, 0, 1), ("z_piece", 4), ("x_send", 4))
    gather(("z_group", 2, 2, 3), ("x_far", -1), ("x_far", 1), ("x_piece", -3))
    gather(("pair_done", 0), ("pair_done", 1), ("pair_done", -1))
    own = (chunk(y),)
    mark("project_own")
    project(own, inner, True, False)
    mark("all_first")
    v = nall.at[chunk_half(left_t, 0)]
    wire.arrive(v, all_sem.at[0, 0], left)
    wire.send(v, v, right, all_sem.at[2, 0])
    v = nall.at[chunk_half(right_t, 1)]
    wire.arrive(v, all_sem.at[1, 1], right)
    wire.send(v, v, left, all_sem.at[2, 1])
    gather(("x_piece", 3), ("x_far", -2), ("x_far", 2), ("z_group", 3, 0, 1, 2, 3))
    gather(("x_piece", 4), ("pair_done", 2), ("pair_done", -2))
    mark("project_own2")
    project(own, outer, False, False)
    gather(("x_far", -3),)
    mark("near_wait")
    wire.arrive(nall.at[chunk_half(left_t, 1)], all_sem.at[0, 1], left)
    wire.arrive(nall.at[chunk_half(right_t, 0)], all_sem.at[1, 0], right)

    @pl.when(has_last)
    def _():
        wire.arrive(tail_in, all_sem.at[3, 0], rank_dev(before, 3))

    @pl.when(jnp.logical_not(has_last))
    def _():
        tail_in[...] = jnp.zeros_like(tail_in)

    rim = tail_in[...].astype(F32)
    rim = jnp.concatenate([rim[2 * k : 2 * k + 2] for k in range(16)], axis=1)
    nall[0:16] = jnp.concatenate([jnp.zeros((14, D), F32), rim], axis=0).astype(BF16)
    near = (chunk(left_t), chunk(right_t), pl.ds(0, 16))
    mark("project_near")
    project(near, inner + outer, True, False)
    gather(("x_far", 3), ("z_group", 4, 0, 1, 2, 3), ("x_far", 4))
    gather(("pair_done", 3), ("pair_done", -3), ("pair_done", 4))
    mark("project_rest")
    project(own + near, rest, False, True)
    ffn_near()
    mark("far_wait")
    wire.arrive(nall.at[chunk_half(far_t, 0)], all_sem.at[2, 0], left)
    wire.arrive(nall.at[chunk_half(far_t, 1)], all_sem.at[2, 1], right)
    mark("project_far")
    project((chunk(far_t),), (0, 1, -1, 2, -2, 3, -3, 4), True, True)
    ffn_far()
    channel = ffn_last()
    out[...] = layer_norm(
        ALPHA * nall[chunk(y), :].astype(F32) + channel, scale_two[...]
    ).astype(BF16)
    mark("finish")
    wire.finish()
    mark.end()


def shards(*arrays):
    arrays = [a.reshape(1, -1) if a.ndim == 1 else a for a in arrays]
    for k in (5, 8, 18):
        arrays[k] = arrays[k].T
    dma = pltpu.SemaphoreType.DMA
    loaded = arrays[:16] + arrays[19:]
    scratch = [pltpu.VMEM(a.shape, a.dtype) for a in loaded] + [
        pltpu.VMEM((8, 4, 2, 32, COLS), BF16),
        dma((22,)),
        pltpu.VMEM((16, INNER), BF16),
        pltpu.VMEM((16, STATE), BF16),
        pltpu.VMEM((16, STATE), BF16),
        pltpu.VMEM((ROWS, INNER), BF16),
        pltpu.VMEM((ROWS, STATE), BF16),
        pltpu.VMEM((ROWS, STATE), BF16),
        pltpu.VMEM((ROWS, 128), F32),
        pltpu.VMEM((BLOCKS, 2 * HEADS, BLOCK), F32),
        pltpu.VMEM((ROWS, INNER), F32),
        pltpu.VMEM((ROWS, INNER), F32),
        pltpu.VMEM((BLOCKS, STATE, INNER), F32),
        pltpu.VMEM((BLOCKS, 8, INNER), F32),
        pltpu.VMEM((STATE, INNER), BF16),
        pltpu.VMEM((8, 16, INNER), BF16),
        pltpu.VMEM((8, 4, 128), F32),
        pltpu.VMEM((8, 16, INNER), F32),
        pltpu.VMEM((8, 8, INNER), F32),
        pltpu.VMEM((4, 128), F32),
        pltpu.VMEM((8, 16, INNER), BF16),
        pltpu.VMEM((8, 4, 128), F32),
        pltpu.VMEM((16, INNER), BF16),
        pltpu.VMEM((4, 128), F32),
        pltpu.VMEM((16, INNER), F32),
        pltpu.VMEM((8, 16, INNER), BF16),
        pltpu.VMEM((STATE, INNER), BF16),
        pltpu.VMEM((3, BLOCK, INNER), BF16),
        pltpu.VMEM((2, 64, INNER), BF16),
        pltpu.VMEM((2, BLOCK, INNER), BF16),
        pltpu.VMEM((2, 64, D), BF16),
        pltpu.VMEM((2, 64, D), BF16),
        pltpu.VMEM((BLOCK, D), F32),
        pltpu.VMEM((2, INNER, D), BF16),
        pltpu.VMEM((ROWS + 16, D), BF16),
        pltpu.VMEM((32, 128), BF16),
        pltpu.VMEM((32, 128), BF16),
        pltpu.VMEM((ROWS + 16, 2 * FF), F32),
        pltpu.VMEM((3, BLOCK, D), BF16),
        pltpu.VMEM((2, 64, D), BF16),
        pltpu.VMEM((2, BLOCK, D), BF16),
        pltpu.VMEM((BLOCK, D), F32),
        dma((260,)),
        dma((86,)),
        dma((8,)),
        dma((3,)),
        dma((2, 8)),
        dma((2, 8)),
        dma((8,)),
        dma((12,)),
        dma((4, 4)),
        dma((4, 2)),
        dma((24,)),
    ]
    return pl.pallas_call(
        layer_kernel,
        out_shape=jax.ShapeDtypeStruct((BLOCK, D), BF16),
        in_specs=[pl.BlockSpec(memory_space=pltpu.HBM)] * len(arrays),
        out_specs=pl.BlockSpec(memory_space=pltpu.VMEM),
        scratch_shapes=scratch,
        compiler_params=pltpu.CompilerParams(
            collective_id=0, has_side_effects=True, vmem_limit_bytes=67043328
        ),
    )(*arrays)

def solution(mesh):
    split = Mesh(mesh.devices.reshape(8, 4, 2, mesh.shape["tp"]), ("sp_0", "sp_1", "sp_2", "tp"))
    in_specs = (
        P(SP_TP, None),
        P(SP, "tp"),
        P(SP, "tp"),
        P(SP, "tp"),
        P(SP, "tp"),
        P(SP, "tp"),
        P("tp"),
        P("tp"),
        P(SP, "tp"),
        P("tp"),
        P(None, "tp"),
        P(None, "tp"),
        P(None, "tp"),
        P("tp"),
        P("tp", None),
        P(),
        P(SP, "tp"),
        P(SP, "tp"),
        P("tp", SP),
        P(None, "tp"),
        P(None, "tp"),
        P(),
    )
    out_specs = P(SP_TP, None)
    return jax.shard_map(
        shards, mesh=split, in_specs=in_specs, out_specs=out_specs, check_vma=False
    )
```

```python
import jax
import jax.numpy as jnp
from jax import lax
from jax.experimental import pallas as pl
from jax.experimental.pallas import tpu as pltpu
from jax.sharding import Mesh
from jax.sharding import PartitionSpec as P

HEADS = 8
HEAD_DIM = 64
STATE = 128
BLOCK = 128
BLOCKS = 4
ROWS = BLOCK * BLOCKS
INNER = 512
D = 2048
FF = 1408
COLS = 3 * FF
NA = 1792
EPSILON = 1e-05
ALPHA = 2.0**0.25
SP = ("sp_0", "sp_1", "sp_2")
SP_TP = ("sp_0", "sp_1", "sp_2", "tp")
MESH = pl.DeviceIdType.MESH
F32 = jnp.float32
BF16 = jnp.bfloat16
NT = (((1,), (1,)), ((), ()))


def wrap(value, count):
    return lax.rem(value + 2 * count, count)


class Marks:
    def __init__(self):
        self.scope = None

    def __call__(self, name):
        self.end()
        self.scope = jax.named_scope(name)
        self.scope.__enter__()

    def end(self):
        if self.scope is not None:
            self.scope.__exit__(None, None, None)
            self.scope = None


class Wire:
    def __init__(self, send_sem):
        self.send_sem = send_sem
        self.count = 0
        self.waits = []

    def send(self, src, dst, dev, recv_sem, when=None):
        copy = pltpu.make_async_remote_copy(
            src_ref=src,
            dst_ref=dst,
            send_sem=self.send_sem.at[self.count],
            recv_sem=recv_sem,
            device_id=dev,
            device_id_type=MESH,
        )
        self.count += 1
        if when is None:
            copy.start()
        else:
            pl.when(when)(copy.start)
        self.waits.append((copy, when))

    def arrive(self, dst, recv_sem, dev):
        pltpu.make_async_remote_copy(
            src_ref=dst,
            dst_ref=dst,
            send_sem=self.send_sem.at[0],
            recv_sem=recv_sem,
            device_id=dev,
            device_id_type=MESH,
        ).wait_recv()

    def finish(self):
        for copy, when in self.waits:
            if when is None:
                copy.wait_send()
            else:
                pl.when(when)(copy.wait_send)


def weight_gather(wire, wv, rsem, psem, ids, mark):
    z, x, c, _ = ids
    cols_a, cols_b = pl.ds(0, NA), pl.ds(NA, COLS - NA)
    half, whole = (pl.ds(0, 16), pl.ds(16, 16)), pl.ds(0, 32)
    zp, zm = {"sp_0": wrap(z + 1, 8)}, {"sp_0": wrap(z - 1, 8)}
    xp, xm = {"sp_1": wrap(x + 1, 4)}, {"sp_1": wrap(x - 1, 4)}
    other = {"sp_2": 1 - c}
    xl, xr, xf = wrap(x - 1, 4), wrap(x + 1, 4), wrap(x + 2, 4)

    def pair(off):
        return psem.at[off % 8]

    def piece(zz, xx, cols, rows=whole):
        return wv.at[zz, xx, c, rows, cols]

    def group(zz, rows=whole):
        return wv.at[zz, :, c, rows, cols_a]

    def send(view, dev, sem):
        wire.send(view, view, dev, sem)

    def arrive(view, sem):
        wire.arrive(view, sem, other)

    def a1(d, h):
        return rsem.at[d * 2 + h]

    def a1f(d):
        return rsem.at[4 + d]

    def b1(d, s):
        return rsem.at[14 + d * 4 + s - 1]

    def b2(d, s):
        return rsem.at[22 + d * 8 + s]

    def b2f(d, s):
        return rsem.at[38 + d * 8 + s]

    def a2(d, s, k):
        return rsem.at[54 + d * 16 + (s - 1) * 4 + k]

    columns = (x, xl, xr, xf)

    def x_send(off):
        v = piece(wrap(z + off, 8), x, cols_b)
        send(v, xp, b2(0, off % 8))
        send(v, xm, b2(1, off % 8))

    def start():
        send(piece(z, x, cols_a, half[0]), xp, a1(0, 0))
        send(piece(z, x, cols_a, half[1]), xm, a1(1, 1))
        send(piece(z, x, cols_a, half[1]), xp, a1(0, 1))
        send(piece(z, x, cols_a, half[0]), xm, a1(1, 0))
        send(piece(z, x, cols_b), zp, b1(0, 1))
        send(piece(z, x, cols_b), zm, b1(1, 1))
        send(piece(z, x, cols_a), zp, a2(0, 1, 0))
        send(piece(z, x, cols_a), zm, a2(1, 1, 0))
        send(piece(z, x, cols_b), other, pair(0))

    def row_far():
        v = piece(z, xl, cols_a, half[0])
        arrive(v, a1(0, 0))
        send(v, xp, a1f(0))
        v = piece(z, xr, cols_a, half[1])
        arrive(v, a1(1, 1))
        send(v, xm, a1f(1))

    def row_done():
        arrive(piece(z, xl, cols_a, half[1]), a1(0, 1))
        arrive(piece(z, xr, cols_a, half[0]), a1(1, 0))
        arrive(piece(z, xf, cols_a, half[0]), a1f(0))
        arrive(piece(z, xf, cols_a, half[1]), a1f(1))
        for k in range(1, 4):
            send(piece(z, columns[k], cols_a), zp, a2(0, 1, k))
            send(piece(z, columns[k], cols_a), zm, a2(1, 1, k))
        send(group(z), other, pair(0))

    def z_piece(s):
        zl, zr = wrap(z - s, 8), wrap(z + s, 8)
        if s < 4:
            v = piece(zl, x, cols_b)
            arrive(v, b1(0, s))
            send(v if s < 3 else piece(zl, x, cols_b, half[0]), zp, b1(0, s + 1))
            send(v, other, pair(-s))
            v = piece(zr, x, cols_b)
            arrive(v, b1(1, s))
            send(v if s < 3 else piece(zr, x, cols_b, half[1]), zm, b1(1, s + 1))
            send(v, other, pair(s))
        else:
            arrive(piece(zl, x, cols_b, half[0]), b1(0, 4))
            arrive(piece(zl, x, cols_b, half[1]), b1(1, 4))
            send(piece(zl, x, cols_b), other, pair(4))

    def z_group(s, *which):
        zl, zr = wrap(z - s, 8), wrap(z + s, 8)
        for k in which:
            if s < 4:
                v = piece(zl, columns[k], cols_a)
                arrive(v, a2(0, s, k))
                send(v if s < 3 else piece(zl, columns[k], cols_a, half[0]), zp, a2(0, s + 1, k))
                v = piece(zr, columns[k], cols_a)
                arrive(v, a2(1, s, k))
                send(v if s < 3 else piece(zr, columns[k], cols_a, half[1]), zm, a2(1, s + 1, k))
            else:
                arrive(piece(zl, columns[k], cols_a, half[0]), a2(0, 4, k))
                arrive(piece(zl, columns[k], cols_a, half[1]), a2(1, 4, k))
        if 3 in which:
            send(group(zl), other, pair(-s))
            if s < 4:
                send(group(zr), other, pair(s))

    def x_piece(off):
        zz = wrap(z + off, 8)
        v = piece(zz, xl, cols_b)
        arrive(v, b2(0, off % 8))
        send(piece(zz, xl, cols_b, half[0]), xp, b2f(0, off % 8))
        send(v, other, pair(off))
        v = piece(zz, xr, cols_b)
        arrive(v, b2(1, off % 8))
        send(piece(zz, xr, cols_b, half[1]), xm, b2f(1, off % 8))
        send(v, other, pair(off))

    def x_far(off):
        zz = wrap(z + off, 8)
        arrive(piece(zz, xf, cols_b, half[0]), b2f(0, off % 8))
        arrive(piece(zz, xf, cols_b, half[1]), b2f(1, off % 8))
        send(piece(zz, xf, cols_b), other, pair(off))

    def pair_done(off):
        arrive(wv.at[wrap(z + off, 8), :, 1 - c], pair(off))

    steps = {
        "start": start,
        "row_far": row_far,
        "row_done": row_done,
        "z_piece": z_piece,
        "z_group": z_group,
        "x_send": x_send,
        "x_piece": x_piece,
        "x_far": x_far,
        "pair_done": pair_done,
    }

    def run(*plan):
        for name, *at in plan:
            mark("g_" + name + "".join(str(k) for k in at))
            steps[name](*at)

    return run


def thirds(v):
    high = v.astype(BF16)
    rest = v - high.astype(F32)
    mid = rest.astype(BF16)
    return high, mid, (rest - mid.astype(F32)).astype(BF16)


def dot(a, b):
    return jnp.dot(a, b, preferred_element_type=F32)


def spread(v, onehot):
    return sum(dot(part, onehot) for part in thirds(v))


def silu(v):
    return v * (1.0 / (1.0 + jnp.exp(-v)))


def layer_norm(values, scales):
    centred = values - jnp.mean(values, axis=-1, keepdims=True)
    spread_of = jnp.mean(centred * centred, axis=-1, keepdims=True)
    return centred * lax.rsqrt(spread_of + EPSILON) * scales


LOADED = (
    "resid",
    "valve",
    "x_in",
    "b_in",
    "c_in",
    "deltas",
    "offset",
    "speed",
    "fading",
    "bypass",
    "x_taps",
    "b_taps",
    "c_taps",
    "cluster",
    "w_mix",
    "scale_one",
    "gate_taps",
    "up_taps",
    "scale_two",
)


EARLY = LOADED[2:13]


def layer_kernel(*refs):
    sources, out, refs = refs[:22], refs[22], refs[23:]
    loads, refs = refs[:19], refs[19:]
    (
        resid,
        valve,
        x_in,
        b_in,
        c_in,
        deltas,
        offset,
        speed,
        fading,
        bypass,
        x_taps,
        b_taps,
        c_taps,
        cluster,
        w_mix,
        scale_one,
        gate_taps,
        up_taps,
        scale_two,
    ) = loads
    (
        wv,
        load_sem,
        x_rim,
        b_rim,
        c_rim,
        xs,
        bs,
        cs,
        cums,
        turned,
        ec,
        yw,
        states,
        decays,
        ends,
        row_ends,
        row_decay,
        row_pre,
        row_dpre,
        own_decay,
        z_state,
        z_decay,
        z_out,
        z_dout,
        z_acc,
        to_row,
        incoming,
        gated,
        far_rows,
        near_rows,
        far_out,
        far_got,
        mixed,
        w_near,
        nall,
        tail_out,
        tail_in,
        gu,
        ffn_out,
        ffn_far_in,
        ffn_in,
        ffn_mixed,
        send_sem,
        gather_sem,
        pair_sem,
        rim_sem,
        row_sem,
        z_sem,
        back_sem,
        mix_sem,
        near_sem,
        all_sem,
        ffn_sem,
    ) = refs
    ids = tuple(lax.axis_index(name) for name in SP_TP)
    z, x, c, y = ids
    rank = z * 8 + x * 2 + c
    place = x * 2 + c
    wire = Wire(send_sem)

    def rank_dev(r, tp=None):
        dev = {"sp_0": lax.div(r, 8), "sp_1": lax.div(lax.rem(r, 8), 2), "sp_2": lax.rem(r, 2)}
        if tp is not None:
            dev["tp"] = tp
        return dev

    def row_dev(p):
        return {"sp_1": lax.div(p, 2), "sp_2": lax.rem(p, 2)}

    after, before = wrap(rank + 1, 64), wrap(rank - 1, 64)
    right, left = {"tp": wrap(y + 1, 4)}, {"tp": wrap(y - 1, 4)}

    mark = Marks()
    mark("barrier")
    sem = pltpu.get_barrier_semaphore()
    greeted = [{"sp_0": wrap(z + k, 8)} for k in range(1, 8)]
    greeted += [row_dev(wrap(place + k, 8)) for k in range(1, 8)]
    greeted += [right, left]
    greeted += [rank_dev(before, k) for k in range(4)]
    for dev in greeted:
        pl.semaphore_signal(sem, inc=1, device_id=dev, device_id_type=MESH)

    sources, shards_here = sources[:16] + sources[19:], sources[16:19]
    copies = [
        pltpu.make_async_copy(src, wv.at[z, x, c, :, pl.ds(k * FF, FF)], load_sem.at[19 + k])
        for k, src in enumerate(shards_here)
    ]
    order = sorted(range(19), key=lambda k: LOADED[k] not in EARLY)
    copies += [pltpu.make_async_copy(sources[k], loads[k], load_sem.at[k]) for k in order]
    for copy in copies:
        copy.start()
    for copy in copies[: 3 + len(EARLY)]:
        copy.wait()
    pl.semaphore_wait(sem, len(greeted))

    has_next, has_last = rank < 63, rank > 0
    last = pl.ds(ROWS - 16, 16)
    for k, (src, dst) in enumerate(((x_in, x_rim), (b_in, b_rim), (c_in, c_rim))):
        wire.send(src.at[last], dst, rank_dev(after), rim_sem.at[k], when=has_next)
    gather = weight_gather(wire, wv, gather_sem, pair_sem, ids, mark)
    gather(("start",))
    w_source = sources[LOADED.index("w_mix")]

    def w_rows(core, k):
        return pl.ds(pl.multiple_of(core * 256 + k * 64, 64), 64)

    for k in range(4):
        for d, dev in enumerate((right, left)):
            rows_k = w_rows(c, k)
            wire.send(w_source.at[rows_k], w_near.at[d, rows_k], dev, near_sem.at[d, k])

    def pass_on(k):
        mark("w_pass" + str(k))
        for d, dev in enumerate((left, right)):
            v = w_near.at[d, w_rows(c, k)]
            wire.arrive(v, near_sem.at[d, k], dev)
            wire.send(v, v, {"sp_2": 1 - c}, near_sem.at[2 + d, k])

    def w_whole():
        mark("w_whole")
        for k in range(4):
            for d in range(2):
                wire.arrive(w_near.at[d, w_rows(1 - c, k)], near_sem.at[2 + d, k], {"sp_2": 1 - c})

    rows_at = lax.broadcasted_iota(jnp.int32, (BLOCK, BLOCK), 0)
    cols_at = lax.broadcasted_iota(jnp.int32, (BLOCK, BLOCK), 1)
    causal = rows_at >= cols_at
    triu = (rows_at <= cols_at).astype(BF16)
    onehot = (
        lax.broadcasted_iota(jnp.int32, (HEADS, INNER), 0)
        == lax.div(lax.broadcasted_iota(jnp.int32, (HEADS, INNER), 1), HEAD_DIM)
    ).astype(BF16)
    eye = lax.broadcasted_iota(jnp.int32, (HEADS, HEADS), 0) == lax.broadcasted_iota(
        jnp.int32, (HEADS, HEADS), 1
    )

    def turned_up(v):
        return jnp.sum(
            jnp.where(eye, jnp.broadcast_to(v[...], (HEADS, HEADS)), 0.0), axis=1, keepdims=True
        )

    offset_col, speed_col = turned_up(offset), turned_up(speed)
    skip = spread(jnp.broadcast_to(bypass[...], (8, HEADS)), onehot)[0:1]
    low_lanes = lax.broadcasted_iota(jnp.int32, (BLOCK, 2 * HEAD_DIM), 1) < HEAD_DIM

    def conv_block(src, rim, taps, b):
        if b == 0:
            window = jnp.concatenate([rim[...], src[0:BLOCK]], axis=0).astype(F32)
        else:
            window = src[b * BLOCK - 16 : (b + 1) * BLOCK].astype(F32)
        weights = taps[...].astype(F32)
        total = weights[0:1] * window[13 : 13 + BLOCK]
        for k in range(1, 4):
            total = total + weights[k : k + 1] * window[13 + k : 13 + k + BLOCK]
        return silu(total)

    def local_block(b):
        span = slice(b * BLOCK, (b + 1) * BLOCK)
        x_act = conv_block(x_in, x_rim, x_taps, b).astype(BF16)
        b_act = conv_block(b_in, b_rim, b_taps, b).astype(BF16)
        xs[span] = x_act
        bs[span] = b_act
        raw = deltas[:, span] + offset_col
        step_rows = jnp.maximum(raw, 0.0) + jnp.log1p(jnp.exp(-jnp.abs(raw)))
        cum_rows = spread(fading[:, span] - speed_col * step_rows, triu)
        both = jnp.concatenate([cum_rows, step_rows], axis=0)
        turned[b] = both
        both = jnp.concatenate([both, jnp.zeros((112, BLOCK), F32)], axis=0).T
        cums[span] = both
        cum, step = both[:, 0:HEADS], both[:, HEADS : 2 * HEADS]
        grown = spread(jnp.broadcast_to(jnp.exp(cum[BLOCK - 1 : BLOCK]), (8, HEADS)), onehot)
        to_end = spread(step * jnp.exp(cum[BLOCK - 1 : BLOCK] - cum), onehot)
        weighted = (x_act.astype(F32) * to_end).astype(BF16)
        states[b] = dot(b_act.astype(F32).T.astype(BF16), weighted)
        decays[b] = grown

    def readout_block(b):
        span = slice(b * BLOCK, (b + 1) * BLOCK)
        cs[span] = conv_block(c_in, c_rim, c_taps, b).astype(BF16)
        ec[span] = spread(jnp.exp(cums[span, 0:HEADS]), onehot)

    def within_block(b):
        span = slice(b * BLOCK, (b + 1) * BLOCK)
        affinity = lax.dot_general(cs[span], bs[span], NT, preferred_element_type=F32)
        for pair in range(HEADS // 2):
            lanes = slice(pair * 128, (pair + 1) * 128)
            mixing = []
            for h in (2 * pair, 2 * pair + 1):
                between = cums[span, h : h + 1] - turned[b, h : h + 1]
                lag = jnp.exp(jnp.where(causal, between, -1e30))
                mixing.append((affinity * lag * turned[b, HEADS + h : HEADS + h + 1]).astype(BF16))
            x_pair = xs[span, lanes]
            zero = jnp.zeros_like(x_pair)
            sides = jnp.concatenate(
                [jnp.where(low_lanes, x_pair, zero), jnp.where(low_lanes, zero, x_pair)], axis=0
            )
            yw[span, lanes] = dot(jnp.concatenate(mixing, axis=1), sides) + skip[
                :, lanes
            ] * x_pair.astype(F32)

    def packed(v):
        return jnp.concatenate([v[:, k * 128 : (k + 1) * 128] for k in range(4)], axis=0)

    def unpacked(tile):
        return jnp.concatenate([tile[k : k + 1] for k in range(4)], axis=1)

    mark("local3")
    local_block(3)
    mark("local2")
    local_block(2)
    local_block(1)
    mark("rim_wait")

    @pl.when(has_last)
    def _():
        for k, dst in enumerate((x_rim, b_rim, c_rim)):
            wire.arrive(dst, rim_sem.at[k], rank_dev(before))

    @pl.when(jnp.logical_not(has_last))
    def _():
        for dst in (x_rim, b_rim, c_rim):
            dst[...] = jnp.zeros_like(dst)

    mark("local0")
    local_block(0)
    mark("ends")

    total = jnp.zeros((STATE, INNER), F32)
    growth = jnp.ones((1, INNER), F32)
    for b in range(BLOCKS):
        fresh, decay = states[b], decays[b, 0:1]
        states[b] = total
        decays[b] = jnp.broadcast_to(growth, (8, INNER))
        total = total * decay + fresh
        growth = growth * decay
    ends[...] = total.astype(BF16)
    own_decay[...] = packed(growth)

    def sixteen(p):
        return pl.ds(pl.multiple_of(p * 16, 16), 16)

    for k in range(1, 8):
        to = wrap(place + k, 8)
        wire.send(ends.at[sixteen(to)], row_ends.at[place], row_dev(to), row_sem.at[0, k])
        wire.send(own_decay, row_decay.at[place], row_dev(to), row_sem.at[1, k])
    row_ends[place] = ends[sixteen(place), :]
    row_decay[place] = own_decay[...]
    gather(("row_far",), ("x_send", 0), ("z_piece", 1))
    mark("within01")
    readout_block(0)
    readout_block(1)
    within_block(0)
    within_block(1)
    mark("row_wait")
    for k in range(1, 8):
        src = wrap(place - k, 8)
        wire.arrive(row_ends.at[src], row_sem.at[0, k], row_dev(src))
        wire.arrive(row_decay.at[src], row_sem.at[1, k], row_dev(src))
    pass_on(0)
    mark("row_fold")
    total = jnp.zeros((16, INNER), F32)
    growth = jnp.ones((1, INNER), F32)
    for q in range(8):
        decay = unpacked(row_decay[q])
        row_pre[q] = total
        row_dpre[q] = jnp.broadcast_to(growth, (8, INNER))
        total = total * decay + row_ends[q].astype(F32)
        growth = growth * decay
    z_out[...] = total.astype(BF16)
    z_dout[...] = packed(growth)
    for k in range(1, 8):
        to = {"sp_0": wrap(z + k, 8)}
        wire.send(z_out, z_state.at[k], to, z_sem.at[0, k], when=z + k < 8)
        wire.send(z_dout, z_decay.at[k], to, z_sem.at[1, k], when=z + k < 8)
    gather(("x_send", -1), ("row_done",), ("z_group", 1, 0))
    mark("within23")
    readout_block(2)
    readout_block(3)
    within_block(2)
    within_block(3)
    mark("z_wait")
    z_acc[...] = jnp.zeros_like(z_acc)
    for k in range(7, 0, -1):

        @pl.when(z >= k)
        def _():
            src = {"sp_0": wrap(z - k, 8)}
            wire.arrive(z_state.at[k], z_sem.at[0, k], src)
            wire.arrive(z_decay.at[k], z_sem.at[1, k], src)
            z_acc[...] = z_acc[...] * unpacked(z_decay[k]) + z_state[k].astype(F32)

    mark("z_fold")
    begun = z_acc[...]
    for q in range(8):
        to_row[q] = (begun * row_dpre[q, 0:1] + row_pre[q]).astype(BF16)
    for k in range(1, 8):
        to = wrap(place + k, 8)
        wire.send(to_row.at[to], incoming.at[sixteen(place)], row_dev(to), back_sem.at[k])
    incoming[sixteen(place), :] = to_row[place]
    gather(("x_send", 1), ("x_piece", 0), ("z_piece", 2), ("z_group", 1, 1))
    mark("back_wait")
    for k in range(1, 8):
        src = wrap(place - k, 8)
        wire.arrive(incoming.at[sixteen(src)], back_sem.at[k], row_dev(src))

    for copy in copies[3 + len(EARLY) :]:
        copy.wait()
    turns = [wrap(y + 2, 4), wrap(y + 1, 4), wrap(y - 1, 4), y]

    def gated_block(t):
        span = pl.ds(pl.multiple_of(t * BLOCK, BLOCK), BLOCK)
        begin = states[t] + incoming[...].astype(F32) * decays[t, 0:1]
        gated = yw[span, :] + ec[span, :] * dot(cs[span, :], begin.astype(BF16))
        gated = gated * silu(valve[span, :].astype(F32))
        gated = gated * lax.rsqrt(jnp.mean(gated * gated, axis=-1, keepdims=True) + EPSILON)
        return (gated * cluster[...]).astype(BF16)

    mark("mix_blocks")
    gated[0] = gated_block(turns[0])
    wire.send(gated.at[0, pl.ds(0, 64)], far_rows.at[0], right, mix_sem.at[0])
    wire.send(gated.at[0, pl.ds(64, 64)], far_rows.at[1], left, mix_sem.at[1])
    gated[1] = gated_block(turns[1])
    wire.send(gated.at[1], near_rows.at[0], right, mix_sem.at[2])
    gated[2] = gated_block(turns[2])
    wire.send(gated.at[2], near_rows.at[1], left, mix_sem.at[3])
    pass_on(1)
    pass_on(2)
    mark("mix_own")
    mixed[...] = dot(gated_block(y), w_mix[...])
    gather(("x_send", -2), ("x_send", 2), ("x_piece", -1), ("z_group", 1, 2, 3))
    pass_on(3)
    w_whole()
    mark("mix_far_wait")
    wire.arrive(far_rows.at[0], mix_sem.at[0], left)
    wire.arrive(far_rows.at[1], mix_sem.at[1], right)
    mark("mix_far")
    for j in range(4):
        lanes = pl.ds(j * 512, 512)
        for d, dev in enumerate((right, left)):
            far_out[d, :, j * 512 : (j + 1) * 512] = dot(
                far_rows[d], w_near[d, :, j * 512 : (j + 1) * 512]
            ).astype(BF16)
            wire.send(far_out.at[d, :, lanes], far_got.at[d, :, lanes], dev, mix_sem.at[4 + 4 * d + j])
    gather(("z_piece", 3), ("x_piece", 1), ("x_send", -3), ("x_send", 3))
    mark("mix_near_wait")
    wire.arrive(near_rows.at[0], mix_sem.at[2], left)
    wire.arrive(near_rows.at[1], mix_sem.at[3], right)
    mark("mix_near")
    for d in range(2):
        mixed[...] += dot(near_rows[d], w_near[d])
    gather(("x_piece", -2), ("x_far", 0), ("x_piece", 2), ("z_group", 2, 0, 1))
    gather(("z_piece", 4), ("x_send", 4))
    mark("mix_wait")
    for j in range(4):
        lanes = pl.ds(j * 512, 512)
        for d, dev in enumerate((left, right)):
            wire.arrive(far_got.at[d, :, lanes], mix_sem.at[4 + 4 * d + j], dev)
    mark("norm_one")
    far_sum = jnp.concatenate([far_got[0], far_got[1]], axis=0).astype(F32)
    mixer = mixed[...] + far_sum
    normed = layer_norm(ALPHA * resid[...].astype(F32) + mixer, scale_one[...]).astype(BF16)

    def chunk(t):
        return pl.ds(pl.multiple_of(16 + t * BLOCK, 16), BLOCK)

    def chunk_half(t, h):
        return pl.ds(pl.multiple_of(16 + t * BLOCK + h * 64, 16), 64)

    nall[chunk(y), :] = normed
    tail = normed[BLOCK - 16 :].astype(F32)[14:16]
    tail_out[...] = jnp.concatenate(
        [tail[:, k * 128 : (k + 1) * 128] for k in range(16)], axis=0
    ).astype(BF16)
    for k in range(4):
        wire.send(
            tail_out,
            tail_in,
            rank_dev(after, k),
            all_sem.at[3, 0],
            when=jnp.logical_and(has_next, y == 3),
        )
    mark("all_send")
    for h in range(2):
        for dev, half_of in ((right, h), (left, 1 - h)):
            v = nall.at[chunk_half(y, half_of)]
            wire.send(v, v, dev, all_sem.at[0 if dev is right else 1, half_of])
    def project(spans, offs, first, last_of):
        zs = [wrap(z + off, 8) for off in offs]
        deep = [pl.ds(pl.multiple_of(zz * 256, 256), 256) for zz in zs]
        rows = jnp.concatenate(
            [jnp.concatenate([nall[span, k] for k in deep], axis=1) for span in spans], axis=0
        )

        for j in range(11):
            lanes = slice(j * 256, (j + 1) * 256)
            weights = [wv[zz, :, :, :, lanes].reshape(256, 256) for zz in zs]
            got = dot(rows, jnp.concatenate(weights, axis=0))
            at = 0
            for span in spans:
                mine = got[at : at + span.size]
                at += span.size
                if not first:
                    mine = mine + gu[span, lanes]
                gu[span, lanes] = mine.astype(BF16).astype(F32) if last_of else mine

    far_t, right_t, left_t = turns[0], turns[1], turns[2]
    def hidden_rows(pieces):
        columns = []
        for j in range(11):
            lanes = slice(j * 128, (j + 1) * 128)
            up_lanes = slice(FF + j * 128, FF + (j + 1) * 128)
            rows = []
            for t, first, count in pieces:
                at = pl.ds(pl.multiple_of(t * BLOCK + first + 8, 8), count + 8)
                sums = []
                for source, taps in ((lanes, gate_taps), (up_lanes, up_taps)):
                    window = gu[at, source]
                    weights = taps[:, lanes].astype(F32)
                    total = weights[0:1] * window[6 : 6 + count]
                    for k in range(1, 3):
                        total = total + weights[k : k + 1] * window[6 + k : 6 + k + count]
                    sums.append(total)
                rows.append((silu(sums[0]) * sums[1]).astype(BF16))
            columns.append(rows[0] if len(rows) == 1 else jnp.concatenate(rows, axis=0))
        return jnp.concatenate(columns, axis=1)

    def down(hidden, j):
        w = wv[2 * j : 2 * j + 2, :, :, :, 2 * FF :].reshape(512, FF)
        return lax.dot_general(hidden, w, NT, preferred_element_type=F32)

    upper, lower = pl.ds(0, 64), pl.ds(64, 64)
    tiles = [(j, pl.ds(j * 512, 512), slice(j * 512, (j + 1) * 512)) for j in range(4)]

    def ffn_near():
        mark("ffn_near")
        hidden = hidden_rows(((right_t, 0, 64), (left_t, 64, 64)))
        for j, lanes, at in tiles:
            ffn_out[0, :, at] = down(hidden, j).astype(BF16)
            wire.send(ffn_out.at[0, upper, lanes], ffn_in.at[0, upper, lanes], right, ffn_sem.at[j])
            wire.send(
                ffn_out.at[0, lower, lanes], ffn_in.at[1, lower, lanes], left, ffn_sem.at[4 + j]
            )

    def ffn_far():
        mark("ffn_far")
        hidden = hidden_rows(((far_t, 0, 128),))
        for j, lanes, at in tiles:
            ffn_out[1, :, at] = down(hidden, j).astype(BF16)
            wire.send(ffn_out.at[1, lower, lanes], ffn_far_in.at[0, :, lanes], right, ffn_sem.at[8 + j])
            wire.send(ffn_out.at[1, upper, lanes], ffn_far_in.at[1, :, lanes], left, ffn_sem.at[12 + j])

    def ffn_last():
        mark("ffn_mixed")
        hidden = hidden_rows(((right_t, 64, 64), (left_t, 0, 64)))
        for j, lanes, at in tiles:
            ffn_mixed[:, at] = down(hidden, j)
        mark("ffn_far_wait")
        for j, lanes, at in tiles:
            wire.arrive(ffn_far_in.at[0, :, lanes], ffn_sem.at[8 + j], left)
            wire.arrive(ffn_far_in.at[1, :, lanes], ffn_sem.at[12 + j], right)
            both = jnp.concatenate([ffn_far_in[0, :, at], ffn_far_in[1, :, at]], axis=0)
            ffn_out[2, :, at] = (ffn_mixed[:, at] + both.astype(F32)).astype(BF16)
            wire.send(
                ffn_out.at[2, upper, lanes], ffn_in.at[0, lower, lanes], right, ffn_sem.at[16 + j]
            )
            wire.send(
                ffn_out.at[2, lower, lanes], ffn_in.at[1, upper, lanes], left, ffn_sem.at[20 + j]
            )
        mark("ffn_own")
        hidden = hidden_rows(((y, 0, 128),))
        for j, lanes, at in tiles:
            ffn_mixed[:, at] = down(hidden, j) + ALPHA * nall[chunk(y), at].astype(F32)
        mark("ffn_wait")
        for j, lanes, at in tiles:
            wire.arrive(ffn_in.at[0, upper, lanes], ffn_sem.at[j], left)
            wire.arrive(ffn_in.at[1, lower, lanes], ffn_sem.at[4 + j], right)
        ffn_mixed[0:64] += ffn_in[0, 0:64].astype(F32)
        ffn_mixed[64:] += ffn_in[1, 64:].astype(F32)
        wire.finish()
        for j, lanes, at in tiles:
            wire.arrive(ffn_in.at[0, lower, lanes], ffn_sem.at[16 + j], left)
            wire.arrive(ffn_in.at[1, upper, lanes], ffn_sem.at[20 + j], right)
        mark("norm_two")
        last = jnp.concatenate([ffn_in[1, 0:64], ffn_in[0, 64:]], axis=0)
        return ffn_mixed[...] + last.astype(F32)

    inner, outer = (0, 1, -1), (2, -2)
    rest = (3, -3, 4)
    gather(("z_group", 2, 2, 3), ("x_far", -1), ("x_far", 1), ("x_piece", -3))
    gather(("pair_done", 0), ("pair_done", 1), ("pair_done", -1))
    own = (chunk(y),)
    mark("project_own")
    project(own, inner, True, False)
    gather(("z_group", 3, 0, 1), ("x_piece", 3))
    mark("all_first")
    v = nall.at[chunk_half(left_t, 0)]
    wire.arrive(v, all_sem.at[0, 0], left)
    wire.send(v, v, right, all_sem.at[2, 0])
    v = nall.at[chunk_half(right_t, 1)]
    wire.arrive(v, all_sem.at[1, 1], right)
    wire.send(v, v, left, all_sem.at[2, 1])
    gather(("x_far", -2), ("x_far", 2), ("z_group", 3, 2, 3), ("x_piece", 4))
    gather(("pair_done", 2), ("pair_done", -2))
    mark("project_own2")
    project(own, outer, False, False)
    gather(("x_far", -3),)
    mark("near_wait")
    wire.arrive(nall.at[chunk_half(left_t, 1)], all_sem.at[0, 1], left)
    wire.arrive(nall.at[chunk_half(right_t, 0)], all_sem.at[1, 0], right)

    @pl.when(has_last)
    def _():
        wire.arrive(tail_in, all_sem.at[3, 0], rank_dev(before, 3))

    @pl.when(jnp.logical_not(has_last))
    def _():
        tail_in[...] = jnp.zeros_like(tail_in)

    rim = tail_in[...].astype(F32)
    rim = jnp.concatenate([rim[2 * k : 2 * k + 2] for k in range(16)], axis=1)
    nall[0:16] = jnp.concatenate([jnp.zeros((14, D), F32), rim], axis=0).astype(BF16)
    near = (chunk(left_t), chunk(right_t), pl.ds(0, 16))
    mark("project_near")
    project(near, inner + outer, True, False)
    gather(("x_far", 3), ("z_group", 4, 0, 1, 2, 3), ("x_far", 4))
    gather(("pair_done", 3), ("pair_done", -3), ("pair_done", 4))
    mark("project_rest")
    own_tail = pl.ds(pl.multiple_of(y * BLOCK + BLOCK, 16), 16)
    project(near + (own_tail,), rest, False, True)
    ffn_near()
    mark("project_own3")
    project((pl.ds(pl.multiple_of(y * BLOCK + 16, 16), BLOCK - 16),), rest, False, True)
    mark("far_wait")
    wire.arrive(nall.at[chunk_half(far_t, 0)], all_sem.at[2, 0], left)
    wire.arrive(nall.at[chunk_half(far_t, 1)], all_sem.at[2, 1], right)
    mark("project_far")
    project((chunk(far_t),), (0, 1, -1, 2, -2, 3, -3, 4), True, True)
    ffn_far()
    channel = ffn_last()
    out[...] = layer_norm(channel, scale_two[...]).astype(BF16)
    mark.end()


def shards(*arrays):
    arrays = [a.reshape(1, -1) if a.ndim == 1 else a for a in arrays]
    for k in (5, 8, 18):
        arrays[k] = arrays[k].T
    dma = pltpu.SemaphoreType.DMA
    loaded = arrays[:16] + arrays[19:]
    scratch = [pltpu.VMEM(a.shape, a.dtype) for a in loaded] + [
        pltpu.VMEM((8, 4, 2, 32, COLS), BF16),
        dma((22,)),
        pltpu.VMEM((16, INNER), BF16),
        pltpu.VMEM((16, STATE), BF16),
        pltpu.VMEM((16, STATE), BF16),
        pltpu.VMEM((ROWS, INNER), BF16),
        pltpu.VMEM((ROWS, STATE), BF16),
        pltpu.VMEM((ROWS, STATE), BF16),
        pltpu.VMEM((ROWS, 128), F32),
        pltpu.VMEM((BLOCKS, 2 * HEADS, BLOCK), F32),
        pltpu.VMEM((ROWS, INNER), F32),
        pltpu.VMEM((ROWS, INNER), F32),
        pltpu.VMEM((BLOCKS, STATE, INNER), F32),
        pltpu.VMEM((BLOCKS, 8, INNER), F32),
        pltpu.VMEM((STATE, INNER), BF16),
        pltpu.VMEM((8, 16, INNER), BF16),
        pltpu.VMEM((8, 4, 128), F32),
        pltpu.VMEM((8, 16, INNER), F32),
        pltpu.VMEM((8, 8, INNER), F32),
        pltpu.VMEM((4, 128), F32),
        pltpu.VMEM((8, 16, INNER), BF16),
        pltpu.VMEM((8, 4, 128), F32),
        pltpu.VMEM((16, INNER), BF16),
        pltpu.VMEM((4, 128), F32),
        pltpu.VMEM((16, INNER), F32),
        pltpu.VMEM((8, 16, INNER), BF16),
        pltpu.VMEM((STATE, INNER), BF16),
        pltpu.VMEM((3, BLOCK, INNER), BF16),
        pltpu.VMEM((2, 64, INNER), BF16),
        pltpu.VMEM((2, BLOCK, INNER), BF16),
        pltpu.VMEM((2, 64, D), BF16),
        pltpu.VMEM((2, 64, D), BF16),
        pltpu.VMEM((BLOCK, D), F32),
        pltpu.VMEM((2, INNER, D), BF16),
        pltpu.VMEM((ROWS + 16, D), BF16),
        pltpu.VMEM((32, 128), BF16),
        pltpu.VMEM((32, 128), BF16),
        pltpu.VMEM((ROWS + 16, 2 * FF), F32),
        pltpu.VMEM((3, BLOCK, D), BF16),
        pltpu.VMEM((2, 64, D), BF16),
        pltpu.VMEM((2, BLOCK, D), BF16),
        pltpu.VMEM((BLOCK, D), F32),
        dma((260,)),
        dma((86,)),
        dma((8,)),
        dma((3,)),
        dma((2, 8)),
        dma((2, 8)),
        dma((8,)),
        dma((12,)),
        dma((4, 4)),
        dma((4, 2)),
        dma((24,)),
    ]
    return pl.pallas_call(
        layer_kernel,
        out_shape=jax.ShapeDtypeStruct((BLOCK, D), BF16),
        in_specs=[pl.BlockSpec(memory_space=pltpu.HBM)] * len(arrays),
        out_specs=pl.BlockSpec(memory_space=pltpu.VMEM),
        scratch_shapes=scratch,
        compiler_params=pltpu.CompilerParams(
            collective_id=0, has_side_effects=True, vmem_limit_bytes=67043328
        ),
    )(*arrays)

def solution(mesh):
    split = Mesh(mesh.devices.reshape(8, 4, 2, mesh.shape["tp"]), ("sp_0", "sp_1", "sp_2", "tp"))
    in_specs = (
        P(SP_TP, None),
        P(SP, "tp"),
        P(SP, "tp"),
        P(SP, "tp"),
        P(SP, "tp"),
        P(SP, "tp"),
        P("tp"),
        P("tp"),
        P(SP, "tp"),
        P("tp"),
        P(None, "tp"),
        P(None, "tp"),
        P(None, "tp"),
        P("tp"),
        P("tp", None),
        P(),
        P(SP, "tp"),
        P(SP, "tp"),
        P("tp", SP),
        P(None, "tp"),
        P(None, "tp"),
        P(),
    )
    out_specs = P(SP_TP, None)
    return jax.shard_map(
        shards, mesh=split, in_specs=in_specs, out_specs=out_specs, check_vma=False
    )
```

```python
import jax
import jax.numpy as jnp
from jax import lax
from jax.experimental import pallas as pl
from jax.experimental.pallas import tpu as pltpu
from jax.sharding import Mesh
from jax.sharding import PartitionSpec as P

HEADS = 8
HEAD_DIM = 64
STATE = 128
BLOCK = 128
BLOCKS = 4
ROWS = BLOCK * BLOCKS
INNER = 512
D = 2048
FF = 1408
COLS = 3 * FF
NA = 1792
EPSILON = 1e-05
ALPHA = 2.0**0.25
SP = ("sp_0", "sp_1", "sp_2")
SP_TP = ("sp_0", "sp_1", "sp_2", "tp")
MESH = pl.DeviceIdType.MESH
F32 = jnp.float32
BF16 = jnp.bfloat16
NT = (((1,), (1,)), ((), ()))


def wrap(value, count):
    return lax.rem(value + 2 * count, count)


class Marks:
    def __init__(self):
        self.scope = None

    def __call__(self, name):
        self.end()
        self.scope = jax.named_scope(name)
        self.scope.__enter__()

    def end(self):
        if self.scope is not None:
            self.scope.__exit__(None, None, None)
            self.scope = None


class Wire:
    def __init__(self, send_sem):
        self.send_sem = send_sem
        self.count = 0
        self.waits = []

    def send(self, src, dst, dev, recv_sem, when=None):
        copy = pltpu.make_async_remote_copy(
            src_ref=src,
            dst_ref=dst,
            send_sem=self.send_sem.at[self.count],
            recv_sem=recv_sem,
            device_id=dev,
            device_id_type=MESH,
        )
        self.count += 1
        if when is None:
            copy.start()
        else:
            pl.when(when)(copy.start)
        self.waits.append((copy, when))

    def arrive(self, dst, recv_sem, dev):
        pltpu.make_async_remote_copy(
            src_ref=dst,
            dst_ref=dst,
            send_sem=self.send_sem.at[0],
            recv_sem=recv_sem,
            device_id=dev,
            device_id_type=MESH,
        ).wait_recv()

    def finish(self):
        for copy, when in self.waits:
            if when is None:
                copy.wait_send()
            else:
                pl.when(when)(copy.wait_send)


def weight_gather(wire, wv, rsem, psem, ids, mark):
    z, x, c, _ = ids
    cols_a, cols_b = pl.ds(0, NA), pl.ds(NA, COLS - NA)
    half, whole = (pl.ds(0, 16), pl.ds(16, 16)), pl.ds(0, 32)
    zp, zm = {"sp_0": wrap(z + 1, 8)}, {"sp_0": wrap(z - 1, 8)}
    xp, xm = {"sp_1": wrap(x + 1, 4)}, {"sp_1": wrap(x - 1, 4)}
    other = {"sp_2": 1 - c}
    xl, xr, xf = wrap(x - 1, 4), wrap(x + 1, 4), wrap(x + 2, 4)

    def pair(off):
        return psem.at[off % 8]

    def piece(zz, xx, cols, rows=whole):
        return wv.at[zz, xx, c, rows, cols]

    def group(zz, rows=whole):
        return wv.at[zz, :, c, rows, cols_a]

    def send(view, dev, sem):
        wire.send(view, view, dev, sem)

    def arrive(view, sem):
        wire.arrive(view, sem, other)

    def a1(d, h):
        return rsem.at[d * 2 + h]

    def a1f(d):
        return rsem.at[4 + d]

    def b1(d, s):
        return rsem.at[14 + d * 4 + s - 1]

    def b2(d, s):
        return rsem.at[22 + d * 8 + s]

    def b2f(d, s):
        return rsem.at[38 + d * 8 + s]

    def a2(d, s, k):
        return rsem.at[54 + d * 16 + (s - 1) * 4 + k]

    columns = (x, xl, xr, xf)

    def x_send(off):
        v = piece(wrap(z + off, 8), x, cols_b)
        send(v, xp, b2(0, off % 8))
        send(v, xm, b2(1, off % 8))

    def start():
        send(piece(z, x, cols_a, half[0]), xp, a1(0, 0))
        send(piece(z, x, cols_a, half[1]), xm, a1(1, 1))
        send(piece(z, x, cols_a, half[1]), xp, a1(0, 1))
        send(piece(z, x, cols_a, half[0]), xm, a1(1, 0))
        send(piece(z, x, cols_b), zp, b1(0, 1))
        send(piece(z, x, cols_b), zm, b1(1, 1))
        send(piece(z, x, cols_a), zp, a2(0, 1, 0))
        send(piece(z, x, cols_a), zm, a2(1, 1, 0))
        send(piece(z, x, cols_b), other, pair(0))

    def row_far():
        v = piece(z, xl, cols_a, half[0])
        arrive(v, a1(0, 0))
        send(v, xp, a1f(0))
        v = piece(z, xr, cols_a, half[1])
        arrive(v, a1(1, 1))
        send(v, xm, a1f(1))

    def row_done():
        arrive(piece(z, xl, cols_a, half[1]), a1(0, 1))
        arrive(piece(z, xr, cols_a, half[0]), a1(1, 0))
        arrive(piece(z, xf, cols_a, half[0]), a1f(0))
        arrive(piece(z, xf, cols_a, half[1]), a1f(1))
        for k in range(1, 4):
            send(piece(z, columns[k], cols_a), zp, a2(0, 1, k))
            send(piece(z, columns[k], cols_a), zm, a2(1, 1, k))
        send(group(z), other, pair(0))

    def z_piece(s):
        zl, zr = wrap(z - s, 8), wrap(z + s, 8)
        if s < 4:
            v = piece(zl, x, cols_b)
            arrive(v, b1(0, s))
            send(v if s < 3 else piece(zl, x, cols_b, half[0]), zp, b1(0, s + 1))
            send(v, other, pair(-s))
            v = piece(zr, x, cols_b)
            arrive(v, b1(1, s))
            send(v if s < 3 else piece(zr, x, cols_b, half[1]), zm, b1(1, s + 1))
            send(v, other, pair(s))
        else:
            arrive(piece(zl, x, cols_b, half[0]), b1(0, 4))
            arrive(piece(zl, x, cols_b, half[1]), b1(1, 4))
            send(piece(zl, x, cols_b), other, pair(4))

    def z_group(s, *which):
        zl, zr = wrap(z - s, 8), wrap(z + s, 8)
        for k in which:
            if s < 4:
                v = piece(zl, columns[k], cols_a)
                arrive(v, a2(0, s, k))
                send(v if s < 3 else piece(zl, columns[k], cols_a, half[0]), zp, a2(0, s + 1, k))
                v = piece(zr, columns[k], cols_a)
                arrive(v, a2(1, s, k))
                send(v if s < 3 else piece(zr, columns[k], cols_a, half[1]), zm, a2(1, s + 1, k))
            else:
                arrive(piece(zl, columns[k], cols_a, half[0]), a2(0, 4, k))
                arrive(piece(zl, columns[k], cols_a, half[1]), a2(1, 4, k))
        if 3 in which:
            send(group(zl), other, pair(-s))
            if s < 4:
                send(group(zr), other, pair(s))

    def x_piece(off):
        zz = wrap(z + off, 8)
        v = piece(zz, xl, cols_b)
        arrive(v, b2(0, off % 8))
        send(piece(zz, xl, cols_b, half[0]), xp, b2f(0, off % 8))
        send(v, other, pair(off))
        v = piece(zz, xr, cols_b)
        arrive(v, b2(1, off % 8))
        send(piece(zz, xr, cols_b, half[1]), xm, b2f(1, off % 8))
        send(v, other, pair(off))

    def x_far(off):
        zz = wrap(z + off, 8)
        arrive(piece(zz, xf, cols_b, half[0]), b2f(0, off % 8))
        arrive(piece(zz, xf, cols_b, half[1]), b2f(1, off % 8))
        send(piece(zz, xf, cols_b), other, pair(off))

    def pair_done(off):
        arrive(wv.at[wrap(z + off, 8), :, 1 - c], pair(off))

    steps = {
        "start": start,
        "row_far": row_far,
        "row_done": row_done,
        "z_piece": z_piece,
        "z_group": z_group,
        "x_send": x_send,
        "x_piece": x_piece,
        "x_far": x_far,
        "pair_done": pair_done,
    }

    def run(*plan):
        for name, *at in plan:
            mark("g_" + name + "".join(str(k) for k in at))
            steps[name](*at)

    return run


def thirds(v):
    high = v.astype(BF16)
    rest = v - high.astype(F32)
    mid = rest.astype(BF16)
    return high, mid, (rest - mid.astype(F32)).astype(BF16)


def dot(a, b):
    return jnp.dot(a, b, preferred_element_type=F32)


def spread(v, onehot):
    return sum(dot(part, onehot) for part in thirds(v))


def silu(v):
    return v * (1.0 / (1.0 + jnp.exp(-v)))


def layer_norm(values, scales):
    centred = values - jnp.mean(values, axis=-1, keepdims=True)
    spread_of = jnp.mean(centred * centred, axis=-1, keepdims=True)
    return centred * lax.rsqrt(spread_of + EPSILON) * scales


LOADED = (
    "resid",
    "valve",
    "x_in",
    "b_in",
    "c_in",
    "deltas",
    "offset",
    "speed",
    "fading",
    "bypass",
    "x_taps",
    "b_taps",
    "c_taps",
    "cluster",
    "w_mix",
    "scale_one",
    "gate_taps",
    "up_taps",
    "scale_two",
)


EARLY = LOADED[2:13]


def layer_kernel(*refs):
    sources, out, refs = refs[:22], refs[22], refs[23:]
    loads, refs = refs[:19], refs[19:]
    (
        resid,
        valve,
        x_in,
        b_in,
        c_in,
        deltas,
        offset,
        speed,
        fading,
        bypass,
        x_taps,
        b_taps,
        c_taps,
        cluster,
        w_mix,
        scale_one,
        gate_taps,
        up_taps,
        scale_two,
    ) = loads
    (
        wv,
        load_sem,
        x_rim,
        b_rim,
        c_rim,
        xs,
        bs,
        cs,
        cums,
        turned,
        ec,
        yw,
        states,
        decays,
        ends,
        row_ends,
        row_decay,
        row_pre,
        row_dpre,
        own_decay,
        z_state,
        z_decay,
        z_out,
        z_dout,
        z_acc,
        to_row,
        incoming,
        gated,
        far_rows,
        near_rows,
        far_out,
        far_got,
        mixed,
        w_near,
        nall,
        tail_out,
        tail_in,
        gu,
        ffn_out,
        ffn_far_in,
        ffn_in,
        ffn_mixed,
        send_sem,
        gather_sem,
        pair_sem,
        rim_sem,
        row_sem,
        z_sem,
        back_sem,
        mix_sem,
        near_sem,
        all_sem,
        ffn_sem,
    ) = refs
    ids = tuple(lax.axis_index(name) for name in SP_TP)
    z, x, c, y = ids
    rank = z * 8 + x * 2 + c
    place = x * 2 + c
    wire = Wire(send_sem)

    def rank_dev(r, tp=None):
        dev = {"sp_0": lax.div(r, 8), "sp_1": lax.div(lax.rem(r, 8), 2), "sp_2": lax.rem(r, 2)}
        if tp is not None:
            dev["tp"] = tp
        return dev

    def row_dev(p):
        return {"sp_1": lax.div(p, 2), "sp_2": lax.rem(p, 2)}

    after, before = wrap(rank + 1, 64), wrap(rank - 1, 64)
    right, left = {"tp": wrap(y + 1, 4)}, {"tp": wrap(y - 1, 4)}

    mark = Marks()
    mark("barrier")
    sem = pltpu.get_barrier_semaphore()
    greeted = [{"sp_0": wrap(z + k, 8)} for k in range(1, 8)]
    greeted += [row_dev(wrap(place + k, 8)) for k in range(1, 8)]
    greeted += [right, left]
    greeted += [rank_dev(before, k) for k in range(4)]
    for dev in greeted:
        pl.semaphore_signal(sem, inc=1, device_id=dev, device_id_type=MESH)

    sources, shards_here = sources[:16] + sources[19:], sources[16:19]
    copies = [
        pltpu.make_async_copy(src, wv.at[z, x, c, :, pl.ds(k * FF, FF)], load_sem.at[19 + k])
        for k, src in enumerate(shards_here)
    ]
    order = sorted(range(19), key=lambda k: LOADED[k] not in EARLY)
    copies += [pltpu.make_async_copy(sources[k], loads[k], load_sem.at[k]) for k in order]
    for copy in copies:
        copy.start()
    for copy in copies[:3]:
        copy.wait()
    pl.semaphore_wait(sem, len(greeted))

    has_next, has_last = rank < 63, rank > 0
    last = pl.ds(ROWS - 16, 16)
    for k, dst in enumerate((x_rim, b_rim, c_rim)):
        src = sources[LOADED.index(("x_in", "b_in", "c_in")[k])]
        wire.send(src.at[last], dst, rank_dev(after), rim_sem.at[k], when=has_next)
    gather = weight_gather(wire, wv, gather_sem, pair_sem, ids, mark)
    gather(("start",))
    w_source = sources[LOADED.index("w_mix")]

    def w_rows(core, k):
        return pl.ds(pl.multiple_of(core * 256 + k * 64, 64), 64)

    for k in range(4):
        for d, dev in enumerate((right, left)):
            rows_k = w_rows(c, k)
            wire.send(w_source.at[rows_k], w_near.at[d, rows_k], dev, near_sem.at[d, k])

    for copy in copies[3 : 3 + len(EARLY)]:
        copy.wait()

    def pass_on(k):
        mark("w_pass" + str(k))
        for d, dev in enumerate((left, right)):
            v = w_near.at[d, w_rows(c, k)]
            wire.arrive(v, near_sem.at[d, k], dev)
            wire.send(v, v, {"sp_2": 1 - c}, near_sem.at[2 + d, k])

    def w_whole():
        mark("w_whole")
        for k in range(4):
            for d in range(2):
                wire.arrive(w_near.at[d, w_rows(1 - c, k)], near_sem.at[2 + d, k], {"sp_2": 1 - c})

    rows_at = lax.broadcasted_iota(jnp.int32, (BLOCK, BLOCK), 0)
    cols_at = lax.broadcasted_iota(jnp.int32, (BLOCK, BLOCK), 1)
    causal = rows_at >= cols_at
    triu = (rows_at <= cols_at).astype(BF16)
    onehot = (
        lax.broadcasted_iota(jnp.int32, (HEADS, INNER), 0)
        == lax.div(lax.broadcasted_iota(jnp.int32, (HEADS, INNER), 1), HEAD_DIM)
    ).astype(BF16)
    eye = lax.broadcasted_iota(jnp.int32, (HEADS, HEADS), 0) == lax.broadcasted_iota(
        jnp.int32, (HEADS, HEADS), 1
    )

    def turned_up(v):
        return jnp.sum(
            jnp.where(eye, jnp.broadcast_to(v[...], (HEADS, HEADS)), 0.0), axis=1, keepdims=True
        )

    offset_col, speed_col = turned_up(offset), turned_up(speed)
    skip = spread(jnp.broadcast_to(bypass[...], (8, HEADS)), onehot)[0:1]
    low_lanes = lax.broadcasted_iota(jnp.int32, (BLOCK, 2 * HEAD_DIM), 1) < HEAD_DIM

    def conv_block(src, rim, taps, b):
        if b == 0:
            window = jnp.concatenate([rim[...], src[0:BLOCK]], axis=0).astype(F32)
        else:
            window = src[b * BLOCK - 16 : (b + 1) * BLOCK].astype(F32)
        weights = taps[...].astype(F32)
        total = weights[0:1] * window[13 : 13 + BLOCK]
        for k in range(1, 4):
            total = total + weights[k : k + 1] * window[13 + k : 13 + k + BLOCK]
        return silu(total)

    def local_block(b):
        span = slice(b * BLOCK, (b + 1) * BLOCK)
        x_act = conv_block(x_in, x_rim, x_taps, b).astype(BF16)
        b_act = conv_block(b_in, b_rim, b_taps, b).astype(BF16)
        xs[span] = x_act
        bs[span] = b_act
        raw = deltas[:, span] + offset_col
        step_rows = jnp.maximum(raw, 0.0) + jnp.log1p(jnp.exp(-jnp.abs(raw)))
        cum_rows = spread(fading[:, span] - speed_col * step_rows, triu)
        both = jnp.concatenate([cum_rows, step_rows], axis=0)
        turned[b] = both
        both = jnp.concatenate([both, jnp.zeros((112, BLOCK), F32)], axis=0).T
        cums[span] = both
        cum, step = both[:, 0:HEADS], both[:, HEADS : 2 * HEADS]
        grown = spread(jnp.broadcast_to(jnp.exp(cum[BLOCK - 1 : BLOCK]), (8, HEADS)), onehot)
        to_end = spread(step * jnp.exp(cum[BLOCK - 1 : BLOCK] - cum), onehot)
        weighted = (x_act.astype(F32) * to_end).astype(BF16)
        states[b] = dot(b_act.astype(F32).T.astype(BF16), weighted)
        decays[b] = grown

    def readout_block(b):
        span = slice(b * BLOCK, (b + 1) * BLOCK)
        cs[span] = conv_block(c_in, c_rim, c_taps, b).astype(BF16)
        ec[span] = spread(jnp.exp(cums[span, 0:HEADS]), onehot)

    def within_block(b):
        span = slice(b * BLOCK, (b + 1) * BLOCK)
        affinity = lax.dot_general(cs[span], bs[span], NT, preferred_element_type=F32)
        for pair in range(HEADS // 2):
            lanes = slice(pair * 128, (pair + 1) * 128)
            mixing = []
            for h in (2 * pair, 2 * pair + 1):
                between = cums[span, h : h + 1] - turned[b, h : h + 1]
                lag = jnp.exp(jnp.where(causal, between, -1e30))
                mixing.append((affinity * lag * turned[b, HEADS + h : HEADS + h + 1]).astype(BF16))
            x_pair = xs[span, lanes]
            zero = jnp.zeros_like(x_pair)
            sides = jnp.concatenate(
                [jnp.where(low_lanes, x_pair, zero), jnp.where(low_lanes, zero, x_pair)], axis=0
            )
            yw[span, lanes] = dot(jnp.concatenate(mixing, axis=1), sides) + skip[
                :, lanes
            ] * x_pair.astype(F32)

    def packed(v):
        return jnp.concatenate([v[:, k * 128 : (k + 1) * 128] for k in range(4)], axis=0)

    def unpacked(tile):
        return jnp.concatenate([tile[k : k + 1] for k in range(4)], axis=1)

    mark("local3")
    local_block(3)
    mark("local2")
    local_block(2)
    local_block(1)
    mark("rim_wait")

    @pl.when(has_last)
    def _():
        for k, dst in enumerate((x_rim, b_rim, c_rim)):
            wire.arrive(dst, rim_sem.at[k], rank_dev(before))

    @pl.when(jnp.logical_not(has_last))
    def _():
        for dst in (x_rim, b_rim, c_rim):
            dst[...] = jnp.zeros_like(dst)

    mark("local0")
    local_block(0)
    mark("ends")

    total = jnp.zeros((STATE, INNER), F32)
    growth = jnp.ones((1, INNER), F32)
    for b in range(BLOCKS):
        fresh, decay = states[b], decays[b, 0:1]
        states[b] = total
        decays[b] = jnp.broadcast_to(growth, (8, INNER))
        total = total * decay + fresh
        growth = growth * decay
    ends[...] = total.astype(BF16)
    own_decay[...] = packed(growth)

    def sixteen(p):
        return pl.ds(pl.multiple_of(p * 16, 16), 16)

    for k in range(1, 8):
        to = wrap(place + k, 8)
        wire.send(ends.at[sixteen(to)], row_ends.at[place], row_dev(to), row_sem.at[0, k])
        wire.send(own_decay, row_decay.at[place], row_dev(to), row_sem.at[1, k])
    row_ends[place] = ends[sixteen(place), :]
    row_decay[place] = own_decay[...]
    gather(("row_far",), ("x_send", 0), ("z_piece", 1))
    mark("within01")
    readout_block(0)
    readout_block(1)
    within_block(0)
    within_block(1)
    mark("row_wait")
    for k in range(1, 8):
        src = wrap(place - k, 8)
        wire.arrive(row_ends.at[src], row_sem.at[0, k], row_dev(src))
        wire.arrive(row_decay.at[src], row_sem.at[1, k], row_dev(src))
    pass_on(0)
    mark("row_fold")
    total = jnp.zeros((16, INNER), F32)
    growth = jnp.ones((1, INNER), F32)
    for q in range(8):
        decay = unpacked(row_decay[q])
        row_pre[q] = total
        row_dpre[q] = jnp.broadcast_to(growth, (8, INNER))
        total = total * decay + row_ends[q].astype(F32)
        growth = growth * decay
    z_out[...] = total.astype(BF16)
    z_dout[...] = packed(growth)
    for k in range(1, 8):
        to = {"sp_0": wrap(z + k, 8)}
        wire.send(z_out, z_state.at[k], to, z_sem.at[0, k], when=z + k < 8)
        wire.send(z_dout, z_decay.at[k], to, z_sem.at[1, k], when=z + k < 8)
    gather(("x_send", -1), ("row_done",), ("z_group", 1, 0))
    mark("within23")
    readout_block(2)
    readout_block(3)
    within_block(2)
    within_block(3)
    mark("z_wait")
    z_acc[...] = jnp.zeros_like(z_acc)
    for k in range(7, 0, -1):

        @pl.when(z >= k)
        def _():
            src = {"sp_0": wrap(z - k, 8)}
            wire.arrive(z_state.at[k], z_sem.at[0, k], src)
            wire.arrive(z_decay.at[k], z_sem.at[1, k], src)
            z_acc[...] = z_acc[...] * unpacked(z_decay[k]) + z_state[k].astype(F32)

    mark("z_fold")
    begun = z_acc[...]
    for q in range(8):
        to_row[q] = (begun * row_dpre[q, 0:1] + row_pre[q]).astype(BF16)
    for k in range(1, 8):
        to = wrap(place + k, 8)
        wire.send(to_row.at[to], incoming.at[sixteen(place)], row_dev(to), back_sem.at[k])
    incoming[sixteen(place), :] = to_row[place]
    gather(("x_send", 1), ("x_piece", 0), ("z_piece", 2), ("z_group", 1, 1))
    mark("back_wait")
    for k in range(1, 8):
        src = wrap(place - k, 8)
        wire.arrive(incoming.at[sixteen(src)], back_sem.at[k], row_dev(src))

    for copy in copies[3 + len(EARLY) :]:
        copy.wait()
    turns = [wrap(y + 2, 4), wrap(y + 1, 4), wrap(y - 1, 4), y]

    def gated_block(t):
        span = pl.ds(pl.multiple_of(t * BLOCK, BLOCK), BLOCK)
        begin = states[t] + incoming[...].astype(F32) * decays[t, 0:1]
        gated = yw[span, :] + ec[span, :] * dot(cs[span, :], begin.astype(BF16))
        gated = gated * silu(valve[span, :].astype(F32))
        gated = gated * lax.rsqrt(jnp.mean(gated * gated, axis=-1, keepdims=True) + EPSILON)
        return (gated * cluster[...]).astype(BF16)

    mark("mix_blocks")
    gated[0] = gated_block(turns[0])
    wire.send(gated.at[0, pl.ds(0, 64)], far_rows.at[0], right, mix_sem.at[0])
    wire.send(gated.at[0, pl.ds(64, 64)], far_rows.at[1], left, mix_sem.at[1])
    gated[1] = gated_block(turns[1])
    wire.send(gated.at[1], near_rows.at[0], right, mix_sem.at[2])
    gated[2] = gated_block(turns[2])
    wire.send(gated.at[2], near_rows.at[1], left, mix_sem.at[3])
    pass_on(1)
    pass_on(2)
    mark("mix_own")
    mixed[...] = dot(gated_block(y), w_mix[...])
    gather(("x_send", -2), ("x_send", 2), ("x_piece", -1), ("z_group", 1, 2, 3))
    pass_on(3)
    w_whole()
    mark("mix_far_wait")
    wire.arrive(far_rows.at[0], mix_sem.at[0], left)
    wire.arrive(far_rows.at[1], mix_sem.at[1], right)
    mark("mix_far")
    for j in range(4):
        lanes = pl.ds(j * 512, 512)
        for d, dev in enumerate((right, left)):
            far_out[d, :, j * 512 : (j + 1) * 512] = dot(
                far_rows[d], w_near[d, :, j * 512 : (j + 1) * 512]
            ).astype(BF16)
            wire.send(far_out.at[d, :, lanes], far_got.at[d, :, lanes], dev, mix_sem.at[4 + 4 * d + j])
    gather(("z_piece", 3), ("x_piece", 1), ("x_send", -3), ("x_send", 3))
    mark("mix_near_wait")
    wire.arrive(near_rows.at[0], mix_sem.at[2], left)
    wire.arrive(near_rows.at[1], mix_sem.at[3], right)
    mark("mix_near")
    for d in range(2):
        mixed[...] += dot(near_rows[d], w_near[d])
    gather(("x_piece", -2), ("x_far", 0), ("x_piece", 2), ("z_group", 2, 0, 1))
    gather(("z_piece", 4), ("x_send", 4))
    mark("mix_wait")
    for j in range(4):
        lanes = pl.ds(j * 512, 512)
        for d, dev in enumerate((left, right)):
            wire.arrive(far_got.at[d, :, lanes], mix_sem.at[4 + 4 * d + j], dev)
    mark("norm_one")
    far_sum = jnp.concatenate([far_got[0], far_got[1]], axis=0).astype(F32)
    mixer = mixed[...] + far_sum
    normed = layer_norm(ALPHA * resid[...].astype(F32) + mixer, scale_one[...]).astype(BF16)

    def chunk(t):
        return pl.ds(pl.multiple_of(16 + t * BLOCK, 16), BLOCK)

    def chunk_half(t, h):
        return pl.ds(pl.multiple_of(16 + t * BLOCK + h * 64, 16), 64)

    nall[chunk(y), :] = normed
    tail = normed[BLOCK - 16 :].astype(F32)[14:16]
    tail_out[...] = jnp.concatenate(
        [tail[:, k * 128 : (k + 1) * 128] for k in range(16)], axis=0
    ).astype(BF16)
    for k in range(4):
        wire.send(
            tail_out,
            tail_in,
            rank_dev(after, k),
            all_sem.at[3, 0],
            when=jnp.logical_and(has_next, y == 3),
        )
    mark("all_send")
    for h in range(2):
        for dev, half_of in ((right, h), (left, 1 - h)):
            v = nall.at[chunk_half(y, half_of)]
            wire.send(v, v, dev, all_sem.at[0 if dev is right else 1, half_of])
    def project(spans, offs, first, last_of):
        zs = [wrap(z + off, 8) for off in offs]
        deep = [pl.ds(pl.multiple_of(zz * 256, 256), 256) for zz in zs]
        rows = jnp.concatenate(
            [jnp.concatenate([nall[span, k] for k in deep], axis=1) for span in spans], axis=0
        )

        for j in range(11):
            lanes = slice(j * 256, (j + 1) * 256)
            weights = [wv[zz, :, :, :, lanes].reshape(256, 256) for zz in zs]
            got = dot(rows, jnp.concatenate(weights, axis=0))
            at = 0
            for span in spans:
                mine = got[at : at + span.size]
                at += span.size
                if not first:
                    mine = mine + gu[span, lanes]
                gu[span, lanes] = mine.astype(BF16).astype(F32) if last_of else mine

    far_t, right_t, left_t = turns[0], turns[1], turns[2]
    def hidden_rows(pieces):
        columns = []
        for j in range(11):
            lanes = slice(j * 128, (j + 1) * 128)
            up_lanes = slice(FF + j * 128, FF + (j + 1) * 128)
            rows = []
            for t, first, count in pieces:
                at = pl.ds(pl.multiple_of(t * BLOCK + first + 8, 8), count + 8)
                sums = []
                for source, taps in ((lanes, gate_taps), (up_lanes, up_taps)):
                    window = gu[at, source]
                    weights = taps[:, lanes].astype(F32)
                    total = weights[0:1] * window[6 : 6 + count]
                    for k in range(1, 3):
                        total = total + weights[k : k + 1] * window[6 + k : 6 + k + count]
                    sums.append(total)
                rows.append((silu(sums[0]) * sums[1]).astype(BF16))
            columns.append(rows[0] if len(rows) == 1 else jnp.concatenate(rows, axis=0))
        return jnp.concatenate(columns, axis=1)

    def down(hidden, j):
        w = wv[2 * j : 2 * j + 2, :, :, :, 2 * FF :].reshape(512, FF)
        return lax.dot_general(hidden, w, NT, preferred_element_type=F32)

    upper, lower = pl.ds(0, 64), pl.ds(64, 64)
    tiles = [(j, pl.ds(j * 512, 512), slice(j * 512, (j + 1) * 512)) for j in range(4)]

    def ffn_near():
        mark("ffn_near")
        hidden = hidden_rows(((right_t, 0, 64), (left_t, 64, 64)))
        for j, lanes, at in tiles:
            ffn_out[0, :, at] = down(hidden, j).astype(BF16)
            wire.send(ffn_out.at[0, upper, lanes], ffn_in.at[0, upper, lanes], right, ffn_sem.at[j])
            wire.send(
                ffn_out.at[0, lower, lanes], ffn_in.at[1, lower, lanes], left, ffn_sem.at[4 + j]
            )

    def ffn_far():
        mark("ffn_far")
        hidden = hidden_rows(((far_t, 0, 128),))
        for j, lanes, at in tiles:
            ffn_out[1, :, at] = down(hidden, j).astype(BF16)
            wire.send(ffn_out.at[1, lower, lanes], ffn_far_in.at[0, :, lanes], right, ffn_sem.at[8 + j])
            wire.send(ffn_out.at[1, upper, lanes], ffn_far_in.at[1, :, lanes], left, ffn_sem.at[12 + j])

    def ffn_last():
        mark("ffn_mixed")
        hidden = hidden_rows(((right_t, 64, 64), (left_t, 0, 64)))
        for j, lanes, at in tiles:
            ffn_mixed[:, at] = down(hidden, j)
        mark("ffn_far_wait")
        for j, lanes, at in tiles:
            wire.arrive(ffn_far_in.at[0, :, lanes], ffn_sem.at[8 + j], left)
            wire.arrive(ffn_far_in.at[1, :, lanes], ffn_sem.at[12 + j], right)
            both = jnp.concatenate([ffn_far_in[0, :, at], ffn_far_in[1, :, at]], axis=0)
            ffn_out[2, :, at] = (ffn_mixed[:, at] + both.astype(F32)).astype(BF16)
            wire.send(
                ffn_out.at[2, upper, lanes], ffn_in.at[0, lower, lanes], right, ffn_sem.at[16 + j]
            )
            wire.send(
                ffn_out.at[2, lower, lanes], ffn_in.at[1, upper, lanes], left, ffn_sem.at[20 + j]
            )
        mark("ffn_own")
        hidden = hidden_rows(((y, 0, 128),))
        for j, lanes, at in tiles:
            ffn_mixed[:, at] = down(hidden, j) + ALPHA * nall[chunk(y), at].astype(F32)
        mark("ffn_wait")
        for j, lanes, at in tiles:
            wire.arrive(ffn_in.at[0, upper, lanes], ffn_sem.at[j], left)
            wire.arrive(ffn_in.at[1, lower, lanes], ffn_sem.at[4 + j], right)
        ffn_mixed[0:64] += ffn_in[0, 0:64].astype(F32)
        ffn_mixed[64:] += ffn_in[1, 64:].astype(F32)
        wire.finish()
        for j, lanes, at in tiles:
            wire.arrive(ffn_in.at[0, lower, lanes], ffn_sem.at[16 + j], left)
            wire.arrive(ffn_in.at[1, upper, lanes], ffn_sem.at[20 + j], right)
        mark("norm_two")
        last = jnp.concatenate([ffn_in[1, 0:64], ffn_in[0, 64:]], axis=0)
        return ffn_mixed[...] + last.astype(F32)

    inner, outer = (0, 1, -1), (2, -2)
    rest = (3, -3, 4)
    gather(("z_group", 2, 2, 3), ("x_far", -1), ("x_far", 1), ("x_piece", -3))
    gather(("pair_done", 0), ("pair_done", 1), ("pair_done", -1))
    own = (chunk(y),)
    mark("project_own")
    project(own, inner, True, False)
    gather(("z_group", 3, 0, 1), ("x_piece", 3))
    mark("all_first")
    v = nall.at[chunk_half(left_t, 0)]
    wire.arrive(v, all_sem.at[0, 0], left)
    wire.send(v, v, right, all_sem.at[2, 0])
    v = nall.at[chunk_half(right_t, 1)]
    wire.arrive(v, all_sem.at[1, 1], right)
    wire.send(v, v, left, all_sem.at[2, 1])
    gather(("x_far", -2), ("x_far", 2), ("z_group", 3, 2, 3), ("x_piece", 4))
    gather(("pair_done", 2), ("pair_done", -2))
    mark("project_own2")
    project(own, outer, False, False)
    gather(("x_far", -3),)
    mark("near_wait")
    wire.arrive(nall.at[chunk_half(left_t, 1)], all_sem.at[0, 1], left)
    wire.arrive(nall.at[chunk_half(right_t, 0)], all_sem.at[1, 0], right)

    @pl.when(has_last)
    def _():
        wire.arrive(tail_in, all_sem.at[3, 0], rank_dev(before, 3))

    @pl.when(jnp.logical_not(has_last))
    def _():
        tail_in[...] = jnp.zeros_like(tail_in)

    rim = tail_in[...].astype(F32)
    rim = jnp.concatenate([rim[2 * k : 2 * k + 2] for k in range(16)], axis=1)
    nall[0:16] = jnp.concatenate([jnp.zeros((14, D), F32), rim], axis=0).astype(BF16)
    near = (chunk(left_t), chunk(right_t), pl.ds(0, 16))
    mark("project_near")
    project(near, inner + outer, True, False)
    gather(("x_far", 3), ("z_group", 4, 0, 1, 2, 3), ("x_far", 4))
    gather(("pair_done", 3), ("pair_done", -3), ("pair_done", 4))
    mark("project_rest")
    own_tail = pl.ds(pl.multiple_of(y * BLOCK + BLOCK, 16), 16)
    project(near + (own_tail,), rest, False, True)
    ffn_near()
    mark("project_own3")
    project((pl.ds(pl.multiple_of(y * BLOCK + 16, 16), BLOCK - 16),), rest, False, True)
    mark("far_wait")
    wire.arrive(nall.at[chunk_half(far_t, 0)], all_sem.at[2, 0], left)
    wire.arrive(nall.at[chunk_half(far_t, 1)], all_sem.at[2, 1], right)
    mark("project_far")
    project((chunk(far_t),), (0, 1, -1, 2, -2, 3, -3, 4), True, True)
    ffn_far()
    channel = ffn_last()
    out[...] = layer_norm(channel, scale_two[...]).astype(BF16)
    mark.end()


def shards(*arrays):
    arrays = [a.reshape(1, -1) if a.ndim == 1 else a for a in arrays]
    for k in (5, 8, 18):
        arrays[k] = arrays[k].T
    dma = pltpu.SemaphoreType.DMA
    loaded = arrays[:16] + arrays[19:]
    scratch = [pltpu.VMEM(a.shape, a.dtype) for a in loaded] + [
        pltpu.VMEM((8, 4, 2, 32, COLS), BF16),
        dma((22,)),
        pltpu.VMEM((16, INNER), BF16),
        pltpu.VMEM((16, STATE), BF16),
        pltpu.VMEM((16, STATE), BF16),
        pltpu.VMEM((ROWS, INNER), BF16),
        pltpu.VMEM((ROWS, STATE), BF16),
        pltpu.VMEM((ROWS, STATE), BF16),
        pltpu.VMEM((ROWS, 128), F32),
        pltpu.VMEM((BLOCKS, 2 * HEADS, BLOCK), F32),
        pltpu.VMEM((ROWS, INNER), F32),
        pltpu.VMEM((ROWS, INNER), F32),
        pltpu.VMEM((BLOCKS, STATE, INNER), F32),
        pltpu.VMEM((BLOCKS, 8, INNER), F32),
        pltpu.VMEM((STATE, INNER), BF16),
        pltpu.VMEM((8, 16, INNER), BF16),
        pltpu.VMEM((8, 4, 128), F32),
        pltpu.VMEM((8, 16, INNER), F32),
        pltpu.VMEM((8, 8, INNER), F32),
        pltpu.VMEM((4, 128), F32),
        pltpu.VMEM((8, 16, INNER), BF16),
        pltpu.VMEM((8, 4, 128), F32),
        pltpu.VMEM((16, INNER), BF16),
        pltpu.VMEM((4, 128), F32),
        pltpu.VMEM((16, INNER), F32),
        pltpu.VMEM((8, 16, INNER), BF16),
        pltpu.VMEM((STATE, INNER), BF16),
        pltpu.VMEM((3, BLOCK, INNER), BF16),
        pltpu.VMEM((2, 64, INNER), BF16),
        pltpu.VMEM((2, BLOCK, INNER), BF16),
        pltpu.VMEM((2, 64, D), BF16),
        pltpu.VMEM((2, 64, D), BF16),
        pltpu.VMEM((BLOCK, D), F32),
        pltpu.VMEM((2, INNER, D), BF16),
        pltpu.VMEM((ROWS + 16, D), BF16),
        pltpu.VMEM((32, 128), BF16),
        pltpu.VMEM((32, 128), BF16),
        pltpu.VMEM((ROWS + 16, 2 * FF), F32),
        pltpu.VMEM((3, BLOCK, D), BF16),
        pltpu.VMEM((2, 64, D), BF16),
        pltpu.VMEM((2, BLOCK, D), BF16),
        pltpu.VMEM((BLOCK, D), F32),
        dma((260,)),
        dma((86,)),
        dma((8,)),
        dma((3,)),
        dma((2, 8)),
        dma((2, 8)),
        dma((8,)),
        dma((12,)),
        dma((4, 4)),
        dma((4, 2)),
        dma((24,)),
    ]
    return pl.pallas_call(
        layer_kernel,
        out_shape=jax.ShapeDtypeStruct((BLOCK, D), BF16),
        in_specs=[pl.BlockSpec(memory_space=pltpu.HBM)] * len(arrays),
        out_specs=pl.BlockSpec(memory_space=pltpu.VMEM),
        scratch_shapes=scratch,
        compiler_params=pltpu.CompilerParams(
            collective_id=0, has_side_effects=True, vmem_limit_bytes=67043328
        ),
    )(*arrays)

def solution(mesh):
    split = Mesh(mesh.devices.reshape(8, 4, 2, mesh.shape["tp"]), ("sp_0", "sp_1", "sp_2", "tp"))
    in_specs = (
        P(SP_TP, None),
        P(SP, "tp"),
        P(SP, "tp"),
        P(SP, "tp"),
        P(SP, "tp"),
        P(SP, "tp"),
        P("tp"),
        P("tp"),
        P(SP, "tp"),
        P("tp"),
        P(None, "tp"),
        P(None, "tp"),
        P(None, "tp"),
        P("tp"),
        P("tp", None),
        P(),
        P(SP, "tp"),
        P(SP, "tp"),
        P("tp", SP),
        P(None, "tp"),
        P(None, "tp"),
        P(),
    )
    out_specs = P(SP_TP, None)
    return jax.shard_map(
        shards, mesh=split, in_specs=in_specs, out_specs=out_specs, check_vma=False
    )
```
